32 devices in a mesh: sp: 8 (over z, x), tp: 4 (over y, core).
Axes of the slice: x: 2, y: 2, z: 4, core: 2. Of those that a mesh axis runs over, the one named last changes fastest.
Arguments:
- x_in: bfloat16 [8, 3072, 2048], P('tp', 'sp'), may hold values from -13 to 13
- x_new: bfloat16 [8, 2048], P('sp'), may hold values from -6 to 6
- w_x: bfloat16 [2048, 2048], replicated, may hold values from -0.125 to 0.125
- w_b: bfloat16 [2048, 1024], replicated, may hold values from -0.125 to 0.125
- w_c: bfloat16 [2048, 1024], replicated, may hold values from -0.125 to 0.125
- w_dt: bfloat16 [2048, 32], replicated, may hold values from -0.125 to 0.125
- w_z: bfloat16 [2048, 2048], P(None, 'tp'), may hold values from -3 to 3
- conv_w: float32 [4, 4096], replicated, may hold values from -3 to 3
- conv_b: float32 [4096], replicated, may hold values from -3 to 3
- dt_bias: float32 [32], replicated, may hold values from -4 to -2
- a_log: float32 [32], replicated, may hold values from -12 to 0
- d_skip: float32 [32], replicated, may hold values from 1 to 8
- norm_g: float32 [32, 64], P('tp'), may hold values from 0.1 to 1.9
Outputs:
- state_cache: bfloat16 [8, 32, 64, 128], P('sp', 'tp')
- read_out: bfloat16 [8, 32, 64], P('sp', 'tp')
The draws below stay inside these ranges and needn't reach their ends.
All inputs are finite; a program needn't handle non-finite values.
Results may differ from the reference program's by a relative error of at most 0.015.
Values may be sent and summed in bfloat16 or wider, within the bound.
A program may use at most 128 MiB of HBM per device.

```python
import math
import jax
import jax.numpy as jnp
from jax import lax

D = 2048
H = 32
P_SIZE = 64
G = 8
N = 128
KW = 4
POS_DEV = 384
R = 4
SEQS = 8
LENGTH = 3072


def draw_x_in(key, part):
    normal_key, factor_key = jax.random.split(key)
    blocks = LENGTH // POS_DEV
    factor = jnp.exp(jax.random.uniform(factor_key, (SEQS, blocks, 1), jnp.float32, -1.2, 1.2))
    factor = jnp.repeat(factor, POS_DEV, axis=1)
    values = jnp.clip(jax.random.normal(normal_key, (SEQS, LENGTH, D), jnp.float32), -3.9, 3.9) * factor
    return values.astype(jnp.bfloat16)


def draw_a_log(key, part):
    pick_key, fast_key, slow_key = jax.random.split(key, 3)
    pick_draw = jax.random.uniform(pick_key, (H,), jnp.float32)
    fast_share = 0.5
    fast_mag = jnp.exp(jax.random.uniform(fast_key, (H,), jnp.float32, math.log(0.15), math.log(0.5)))
    slow_mag = jnp.exp(jax.random.uniform(slow_key, (H,), jnp.float32, math.log(5.0 / LENGTH), math.log(15.0 / LENGTH)))
    return jnp.log(jnp.where(pick_draw < fast_share, fast_mag, slow_mag)).astype(jnp.float32)


def draw_w_z(key, part):
    entry_key, scale_key = jax.random.split(key)
    col_scale = jnp.exp(jax.random.uniform(scale_key, (1, H * P_SIZE), jnp.float32, -1.2, 1.2))
    entries = jnp.clip(jax.random.normal(entry_key, (D, H * P_SIZE), jnp.float32), -6.0, 6.0)
    return (entries * col_scale * D ** (-0.5)).astype(jnp.bfloat16)


def level_of(key, extent, cuts, least, largest):
    factor_of = 1.0
    for dim, blocks in cuts:
        draws = jax.random.uniform(jax.random.fold_in(jax.random.fold_in(key, 6), dim), (blocks,), jnp.float32, least / len(cuts), largest / len(cuts))
        factor_of = factor_of * jnp.repeat(jnp.exp(draws), extent[dim] // blocks).reshape((-1,) + (1,) * (len(extent) - 1 - dim))
    return factor_of


def noise(rng, dims, width, limit, shards=(), dtype=jnp.bfloat16):
    factor_of = level_of(rng, dims, shards, -0.22, 0.18) if shards else 1.0
    array = jax.random.normal(rng, dims, jnp.float32) * width * factor_of
    return jnp.minimum(jnp.maximum(array, -limit), limit).astype(dtype)


def setup_inputs(seed: int = 0) -> dict:
    key_of = jax.random.split(jax.random.key(seed), 14)
    x_in = draw_x_in(jax.random.fold_in(key_of[13], 71), 0)
    x_new = noise(key_of[1], (SEQS, D), 1.0, 6.0, ((0, 8),))
    w_x = noise(key_of[2], (D, H * P_SIZE), D ** -0.5, 0.125)
    w_b = noise(key_of[3], (D, G * N), D ** -0.5, 0.125)
    w_c = noise(key_of[4], (D, G * N), D ** -0.5, 0.125)
    w_dt = noise(key_of[5], (D, H), D ** -0.5, 0.125)
    w_z = draw_w_z(jax.random.fold_in(key_of[13], 71), 0)
    conv_w = noise(key_of[7], (KW, H * P_SIZE + 2 * G * N), 0.5, 3.0, (), jnp.float32)
    conv_b = noise(key_of[8], (H * P_SIZE + 2 * G * N,), 0.5, 3.0, (), jnp.float32)
    dt_bias = jnp.clip(jax.random.uniform(key_of[9], (H,), jnp.float32, -4.0, -2.0), -4.0, -2.0)
    a_log = draw_a_log(jax.random.fold_in(key_of[13], 71), 0)
    d_skip = jnp.clip(jnp.exp(jax.random.uniform(key_of[11], (H,), jnp.float32, math.log(1.0), math.log(8.0))), 1.0, 8.0)
    norm_g = jnp.clip(1.0 + 0.18 * jax.random.normal(key_of[12], (H, P_SIZE), jnp.float32), 0.1, 1.9)
    return {"x_in": x_in, "x_new": x_new, "w_x": w_x, "w_b": w_b, "w_c": w_c, "w_dt": w_dt, "w_z": w_z, "conv_w": conv_w, "conv_b": conv_b, "dt_bias": dt_bias, "a_log": a_log, "d_skip": d_skip, "norm_g": norm_g}


eps = 1e-05

def shift_conv(padded, weights, biases, col_count):
    acc_sum = biases + jnp.zeros(padded.shape[:1] + (col_count,) + padded.shape[2:], jnp.float32)
    for offset in range(KW):
        acc_sum = acc_sum + weights[offset] * padded[:, offset:offset + col_count].astype(jnp.float32)
    return jax.nn.silu(acc_sum).astype(jnp.bfloat16)

def reference(x_in, x_new, w_x, w_b, w_c, w_dt, w_z, conv_w, conv_b, dt_bias, a_log, d_skip, norm_g):
    inner_cols = H * P_SIZE
    state_cols = G * N
    edge_rows = KW - 1
    decay_rates = -jnp.exp(a_log)

    def one_sequence(token_rows):
        pre_values = jnp.dot(token_rows, w_x, preferred_element_type=jnp.float32).astype(jnp.bfloat16)
        pre_keys = jnp.dot(token_rows, w_b, preferred_element_type=jnp.float32).astype(jnp.bfloat16)
        raw_steps = jnp.dot(token_rows, w_dt, preferred_element_type=jnp.float32).astype(jnp.bfloat16)
        joined = jnp.concatenate([pre_values, pre_keys], axis=1)
        padded = jnp.concatenate([jnp.zeros((edge_rows, joined.shape[1]), jnp.bfloat16), joined], axis=0)
        conved = shift_conv(padded[None], conv_w[:, :inner_cols + state_cols], conv_b[:inner_cols + state_cols], LENGTH)[0]
        step_sizes = jax.nn.softplus(raw_steps.astype(jnp.float32) + dt_bias)
        rest_sum = lax.cumsum(step_sizes, axis=0, reverse=True) - step_sizes
        weight = jnp.exp(decay_rates * rest_sum) * step_sizes
        scaled = (weight[:, :, None] * conved[:, :inner_cols].astype(jnp.float32).reshape(LENGTH, H, P_SIZE)).astype(jnp.bfloat16)
        key_rows = conved[:, inner_cols:].astype(jnp.float32).reshape(LENGTH, G, N)
        state = jnp.einsum('lgrp,lgn->grpn', scaled.astype(jnp.float32).reshape(LENGTH, G, R, P_SIZE), key_rows, precision=lax.Precision.HIGHEST).reshape(H, P_SIZE, N)
        pre_query = jnp.dot(token_rows[LENGTH - edge_rows:], w_c, preferred_element_type=jnp.float32).astype(jnp.bfloat16)
        tail_rows = jnp.concatenate([joined[LENGTH - edge_rows:], pre_query], axis=1)
        return (state, tail_rows)
    states, tails = lax.map(one_sequence, x_in)
    new_pre = jnp.concatenate([jnp.dot(x_new, w_x, preferred_element_type=jnp.float32).astype(jnp.bfloat16), jnp.dot(x_new, w_b, preferred_element_type=jnp.float32).astype(jnp.bfloat16), jnp.dot(x_new, w_c, preferred_element_type=jnp.float32).astype(jnp.bfloat16)], axis=1)
    new_raw = jnp.dot(x_new, w_dt, preferred_element_type=jnp.float32).astype(jnp.bfloat16)
    gate_new = jnp.dot(x_new, w_z, preferred_element_type=jnp.float32).astype(jnp.bfloat16)
    padded = jnp.concatenate([tails, new_pre[:, None, :]], axis=1)
    new_conv = shift_conv(padded, conv_w, conv_b, 1)[:, 0]
    new_values = new_conv[:, :inner_cols].astype(jnp.float32).reshape(SEQS, G, R, P_SIZE)
    new_keys = new_conv[:, inner_cols:inner_cols + state_cols].astype(jnp.float32).reshape(SEQS, G, N)
    new_query = new_conv[:, inner_cols + state_cols:].astype(jnp.float32).reshape(SEQS, G, N)
    new_steps = jax.nn.softplus(new_raw.astype(jnp.float32) + dt_bias)
    decay_new = jnp.exp(decay_rates * new_steps).reshape(SEQS, G, R)
    held_read = jnp.einsum('sgrpn,sgn->sgrp', states.reshape(SEQS, G, R, P_SIZE, N), new_query, precision=lax.Precision.HIGHEST)
    inner_prod = lax.optimization_barrier(jnp.sum(new_query * new_keys, axis=-1))
    step_group = new_steps.reshape(SEQS, G, R)
    output = decay_new[..., None] * held_read + (step_group * inner_prod[:, :, None])[..., None] * new_values + d_skip.reshape(G, R)[None, :, :, None] * new_values
    gated_out = output * jax.nn.silu(gate_new.astype(jnp.float32).reshape(SEQS, G, R, P_SIZE))
    group_ms = lax.optimization_barrier(jnp.mean(gated_out * gated_out, axis=(2, 3)))
    read_out = gated_out * lax.rsqrt(group_ms + eps)[:, :, None, None] * norm_g.reshape(G, R, P_SIZE)
    return (states.astype(jnp.bfloat16), read_out.astype(jnp.bfloat16).reshape(SEQS, H, P_SIZE))
```

```python
import functools

import jax
import jax.numpy as jnp
from jax import lax
from jax.experimental import pallas as pl
from jax.experimental.pallas import tpu as pltpu
from jax.sharding import PartitionSpec as P

MESH = pl.DeviceIdType.MESH
F32 = jnp.float32
BF16 = jnp.bfloat16
EPS = 1e-05
EDGE = 16
SENT = 8
PAIR = 2
LANES = 128


def silu(x):
    half = 0.5 * x
    return half + half * jnp.tanh(half)


def silu_twice(half):
    return half + half * jnp.tanh(half)


def softplus(x):
    return jnp.maximum(x, 0.0) + jnp.log1p(jnp.exp(-jnp.abs(x)))


def rounded(x):
    return x.astype(BF16).astype(F32)


def kernel(
    dims,
    x_ref, xn_ref, wx_ref, wb_ref, wc_ref, wdt_ref, wz_ref,
    cw_hbm, cb_hbm, dtb_ref, alog_ref, dskip_ref, ng_ref,
    state_ref, read_ref,
    xs, wxs, wbs, wdts, wcn, wzn, nt, pre_s0, pre_s1, pre_o0, pre_o1, padded, later, rows, keys, scaled,
    wt, tot_out, tot_in, fcol, a_out, a_in, mine, b_in, st_out, st_in, head_s, read_s, cw_ref, cb_ref,
    x_sem, wdt_sem, w_sem, new_sem, conv_sem, halo_send, halo_recv, tail_send, tail_recv,
    tot_send, tot_recv, a_send, a_recv, b_send, b_recv, st_send, st_recv,
):
    sp, tp, heads, groups, n_size, p_size, ratio, taps = dims
    i, j = lax.axis_index("sp"), lax.axis_index("tp")
    spt, length, _ = x_ref.shape
    hl, gl = heads // tp, groups // tp
    inner, keys_all = heads * p_size, groups * n_size
    gcols = ratio * p_size
    steps = groups // PAIR
    home = i // spt
    pres = ((pre_s0, pre_s1), (pre_o0, pre_o1))
    member, m = lax.rem(i, 2), i // 2
    direct = m // 2 == j // 2
    near = jnp.logical_not(direct) & ((j > m) == (lax.rem(m, 2) == 1))
    far = jnp.logical_not(direct) & jnp.logical_not(near)
    partner, sibling = i + 1 - 2 * member, i + 2 - 4 * lax.rem(m, 2)
    pairs = sp // 4
    after = lax.rem(i + 1, sp)
    starts = (0, length + EDGE)
    seqs = (1 - member, member)
    width_v, width_k, width_h = PAIR * gcols, PAIR * n_size, PAIR * ratio
    vtiles, ktiles = width_v // LANES, width_k // LANES
    tiles_group = gcols // LANES
    heads_tile = LANES // p_size

    def place(s):
        return lax.rem(s + 1 + (j * gl) // PAIR, steps)

    x_copies = [
        pltpu.make_async_copy(x_ref.at[seqs[r]], xs.at[pl.ds(starts[r], length)], x_sem.at[r])
        for r in range(spt)
    ]
    wdt_copy = pltpu.make_async_copy(wdt_ref, wdts, wdt_sem)

    def w_copies(s):
        at = place(s)
        return (
            pltpu.make_async_copy(
                wx_ref.at[:, pl.ds(pl.multiple_of(at * width_v, LANES), width_v)], wxs.at[s], w_sem.at[s, 0]),
            pltpu.make_async_copy(
                wb_ref.at[:, pl.ds(pl.multiple_of(at * width_k, LANES), width_k)], wbs.at[s], w_sem.at[s, 1]),
        )

    vcol = pl.multiple_of(j * (hl * p_size), LANES)
    gcol = pl.multiple_of(j * (gl * n_size), LANES)
    new_copies = [
        pltpu.make_async_copy(wc_ref.at[:, pl.ds(gcol, gl * n_size)], wcn, new_sem.at[0]),
        pltpu.make_async_copy(wz_ref, wzn, new_sem.at[1]),
    ]
    conv_copies = [
        pltpu.make_async_copy(cw_hbm, cw_ref, conv_sem.at[0]),
        pltpu.make_async_copy(cb_hbm, cb_ref, conv_sem.at[1]),
    ]
    wdt_copy.start()
    for c in x_copies:
        c.start()
    for c in w_copies(0):
        c.start()

    barrier = pltpu.get_barrier_semaphore()
    for k in range(sp):
        @pl.when(i != k)
        def _():
            pl.semaphore_signal(barrier, inc=1, device_id={"sp": k, "tp": j}, device_id_type=MESH)

        @pl.when(home != j)
        def _():
            pl.semaphore_signal(barrier, inc=1, device_id={"sp": k, "tp": home}, device_id_type=MESH)
    for c in conv_copies:
        c.start()

    nt[0:EDGE - SENT, :] = jnp.zeros((EDGE - SENT, nt.shape[1]), BF16)
    padded[...] = jnp.zeros_like(padded)
    rows[...] = jnp.zeros_like(rows)
    for r in range(spt):
        rows[0:1, r * heads:(r + 1) * heads] = -jnp.exp(alog_ref[...])
        rows[1:2, r * heads:(r + 1) * heads] = dtb_ref[...]

    @pl.when(i == 0)
    def _():
        xs[length:length + EDGE, :] = jnp.zeros((EDGE, xs.shape[1]), BF16)

    before = lax.broadcasted_iota(jnp.int32, (length, length), 0)
    column_at = lax.broadcasted_iota(jnp.int32, (length, length), 1)
    later[...] = (before > column_at).astype(F32).astype(BF16)

    def column(row):
        return jnp.broadcast_to(row, (LANES, LANES)).T

    wdt_copy.wait()
    for c in x_copies:
        c.wait()
    for r in range(spt):
        raw = lax.dot_general(
            xs[starts[r]:starts[r] + length, :], wdts[...], (((1,), (1,)), ((), ())), preferred_element_type=F32)
        padded[r, :, 0:heads] = rounded(raw)

    pl.semaphore_wait(barrier, sp - 1 + spt * (tp - 1))

    def halo(r):
        return pltpu.make_async_remote_copy(
            src_ref=xs.at[pl.ds(starts[r] + length - SENT, SENT)],
            dst_ref=xs.at[pl.ds(length + SENT * (1 - r), SENT)],
            send_sem=halo_send.at[r], recv_sem=halo_recv.at[1 - r],
            device_id={"sp": after, "tp": j}, device_id_type=MESH)

    def tail(r, q):
        src = xs.at[pl.ds(starts[r] + length - SENT, SENT)]
        dst = nt.at[pl.ds(EDGE - SENT, SENT)]
        target = spt * j + seqs[r]
        return (target == i) & (q == j), pltpu.make_async_remote_copy(
            src_ref=src, dst_ref=dst, send_sem=tail_send.at[r, q], recv_sem=tail_recv.at[0],
            device_id={"sp": target, "tp": q}, device_id_type=MESH
        ), pltpu.make_async_copy(src, dst, tail_recv.at[0])

    @pl.when(i != sp - 1)
    def _():
        for r in range(spt):
            halo(r).start()

    @pl.when(i == sp - 1)
    def _():
        for r in range(spt):
            for q in range(tp):
                here, remote, local = tail(r, q)
                pl.when(jnp.logical_not(here))(remote.start)
                pl.when(here)(local.start)

    def tot(k):
        return pltpu.make_async_remote_copy(
            src_ref=tot_out, dst_ref=tot_in.at[i], send_sem=tot_send.at[k], recv_sem=tot_recv.at[i],
            device_id={"sp": k, "tp": j}, device_id_type=MESH)

    def decays():
        turned = jnp.concatenate([padded[r].T[0:heads] for r in range(spt)], axis=0)
        rates = column(rows[0:1, :])[0:spt * heads, 0:1]
        biases = column(rows[1:2, :])[0:spt * heads, 0:1]
        sizes = softplus(turned + biases)
        parts, left = [], sizes
        for _ in range(3):
            parts.append(left.astype(BF16))
            left = left - parts[-1].astype(F32)
        sums = jnp.dot(jnp.concatenate(parts, axis=0), later[...], preferred_element_type=F32)
        rest = sum(sums[k * spt * heads:(k + 1) * spt * heads] for k in range(3))
        weights = jnp.exp(rates * rest) * sizes
        for r in range(spt):
            wt[r] = weights[r * heads:(r + 1) * heads]
        total = jnp.broadcast_to(rest[:, 0:1] + sizes[:, 0:1], (spt * heads, LANES))
        given, kept = total[0:heads], total[heads:2 * heads]
        tots = jnp.concatenate([
            jnp.where(member == 0, kept, given), jnp.where(member == 0, given, kept),
            jnp.zeros((LANES - spt * heads, LANES), F32)], axis=0)
        tot_out[...] = tots.T[0:8]

    def factors():
        for k in range(sp):
            @pl.when(i != k)
            def _():
                pltpu.make_async_remote_copy(
                    src_ref=tot_out, dst_ref=tot_in.at[k], send_sem=tot_send.at[k], recv_sem=tot_recv.at[k],
                    device_id={"sp": k, "tp": j}, device_id_type=MESH).wait_recv()
        for at, who in enumerate((i, partner)):
            beyond = jnp.zeros((1, LANES), F32)
            for k in range(sp):
                beyond = beyond + jnp.where(k > who, tot_in[k, 0:1, :], 0.0)
            both = column(jnp.exp(rows[0:1, :] * beyond))
            fcol[at] = jnp.where(member == 0, both[0:heads], both[heads:2 * heads])

    def a_copy(s, gp):
        return pltpu.make_async_remote_copy(
            src_ref=a_out.at[s, gp], dst_ref=a_in.at[s, gp], send_sem=a_send.at[s, gp], recv_sem=a_recv.at[s, gp],
            device_id={"sp": partner, "tp": j}, device_id_type=MESH)

    def b_copy(s, gp):
        return pltpu.make_async_remote_copy(
            src_ref=st_out.at[s, gp], dst_ref=b_in.at[s, gp], send_sem=b_send.at[s, gp], recv_sem=b_recv.at[s, gp],
            device_id={"sp": sibling, "tp": j}, device_id_type=MESH)

    slot = jnp.where(direct & (lax.rem(m, 2) == 1), pairs, m // 2)

    def state_copy(s, gp):
        g = place(s) * PAIR + gp
        q = g // gl
        src, dst = st_out.at[s, gp], st_in.at[slot, lax.rem(g, gl)]
        sem = st_recv.at[slot, lax.rem(g, gl)]
        return (m == j) & (q == j), pltpu.make_async_remote_copy(
            src_ref=src, dst_ref=dst, send_sem=st_send.at[s, gp], recv_sem=sem,
            device_id={"sp": spt * j + member, "tp": q}, device_id_type=MESH
        ), pltpu.make_async_copy(src, dst, sem)

    def pass_on(s):
        at = pl.multiple_of(place(s) * width_h, width_h)

        def add(gp, *more):
            scales = [fcol[k, pl.ds(at, width_h), :] for k in range(2)]
            for r in range(ratio):
                h, span = gp * ratio + r, slice(r * p_size, (r + 1) * p_size)
                total = scales[0][h:h + 1] * mine[s, gp, span, :]
                total += scales[1][h:h + 1] * a_in[s, gp, span, :].astype(F32)
                for ref in more:
                    total += ref[s, gp, span, :].astype(F32)
                st_out[s, gp, span, :] = total.astype(BF16)

        for gp in range(PAIR):
            a_copy(s, gp).wait_recv()

            @pl.when(near)
            def _():
                b_copy(s, gp).wait_recv()
                add(gp, b_in)

            @pl.when(jnp.logical_not(near))
            def _():
                add(gp)

            @pl.when(far)
            def _():
                b_copy(s, gp).start()

            @pl.when(jnp.logical_not(far))
            def _():
                here, remote, local = state_copy(s, gp)
                pl.when(jnp.logical_not(here))(remote.start)
                pl.when(here)(local.start)

    def project(s, first, count, w, base, tiles, keep):
        cuts = [0, count] if tiles > 2 else [0, count // 2 // EDGE * EDGE, count]
        out = jnp.concatenate([
            jnp.dot(xs[first + lo:first + hi, :], w[s], preferred_element_type=F32)
            for lo, hi in zip(cuts, cuts[1:])], axis=0)
        for c in range(tiles):
            keep(base + c, out[:, c * LANES:(c + 1) * LANES])

    def given_alone(s):
        def keep(c, v):
            pres[0][s % 2][c, SENT:SENT + length, :] = v
        return s, 0, length, keep

    def given_with_edges(s):
        def keep(c, v):
            pres[0][s % 2][c, SENT:SENT + length, :] = v[0:length]
            pres[0][s % 2][c, 0:SENT, :] = v[length:length + SENT]
            pres[1][s % 2][c, 0:SENT, :] = v[length + SENT:length + EDGE]
        return s, 0, length + EDGE, keep

    def kept_with_edges(s):
        def keep(c, v):
            pres[0][s % 2][c, 0:SENT, :] = v[0:SENT]
            pres[1][s % 2][c, :, :] = v[SENT:EDGE + length]
        return s, length, length + EDGE, keep

    def kept_alone(s):
        def keep(c, v):
            pres[1][s % 2][c, SENT:SENT + length, :] = v
        return s, length + EDGE, length, keep

    def values_of(job):
        s, first, count, keep = job
        project(s, first, count, wxs, 0, vtiles, keep)

    def keys_of(job):
        s, first, count, keep = job
        project(s, first, count, wbs, vtiles, ktiles, keep)

    def contract(s, r):
        place_s = place(s)
        pre = pres[r][s % 2]

        def conv(c):
            if c < vtiles:
                at = pl.multiple_of(place_s * width_v + c * LANES, LANES)
            else:
                at = pl.multiple_of(inner + place_s * width_k + (c - vtiles) * LANES, LANES)
            acc = cb_ref[:, pl.ds(at, LANES)]
            w = cw_ref[:, pl.ds(at, LANES)]
            for o in range(taps):
                acc = acc + w[o:o + 1] * pre[c, pl.ds(SENT - taps + 1 + o, length), :]
            return silu_twice(acc).astype(BF16)

        weights = wt[r, pl.ds(pl.multiple_of(place_s * width_h, width_h), width_h), :]
        for gp in range(PAIR):
            keys[r, gp] = conv(vtiles + gp)
            for c in range(gp * tiles_group, (gp + 1) * tiles_group):
                turned = conv(c).T
                for k in range(heads_tile):
                    h = c * heads_tile + k
                    part = turned[k * p_size:(k + 1) * p_size].astype(F32)
                    scaled[r, gp, (h - gp * ratio) * p_size:(h - gp * ratio + 1) * p_size] = (
                        weights[h:h + 1] * part).astype(BF16)

    def combine(s, r):
        for gp in range(PAIR):
            out = jnp.dot(scaled[r, gp], keys[r, gp], preferred_element_type=F32)
            if r == 0:
                a_out[s, gp] = out.astype(BF16)
                a_copy(s, gp).start()
            else:
                mine[s, gp] = out

    def w_wait(s):
        for c in w_copies(s):
            c.wait()

    w_wait(0)
    for c in w_copies(1):
        c.start()
    values_of(given_alone(0))
    decays()
    keys_of(given_alone(0))

    tot_in[i] = tot_out[...]
    for k in range(sp):
        pl.when(i != k)(tot(k).start)

    @pl.when(i != 0)
    def _():
        for r in range(spt):
            halo(r).wait_recv()
    for s in range(2, steps):
        for c in w_copies(s):
            c.start()
    for c in new_copies:
        c.start()
    for c in conv_copies:
        c.wait()
    cw_ref[...] = 0.5 * cw_ref[...]
    cb_ref[...] = 0.5 * cb_ref[...]

    values_of(kept_with_edges(0))
    keys_of(kept_with_edges(0))

    for s in range(steps - 1):
        w_wait(s + 1)
        values_of(given_with_edges(s + 1))
        keys_of(given_with_edges(s + 1))
        contract(s, 0)
        combine(s, 0)
        values_of(kept_alone(s + 1))
        keys_of(kept_alone(s + 1))
        contract(s, 1)
        combine(s, 1)
        if s == 1:
            factors()
        if s > 0:
            pl.when(jnp.logical_not(near))(functools.partial(pass_on, s - 1))
    contract(steps - 1, 0)
    combine(steps - 1, 0)
    contract(steps - 1, 1)
    combine(steps - 1, 1)
    pl.when(near)(lambda: pass_on(0))

    newest = jnp.broadcast_to(xn_ref[...].astype(F32), (EDGE, xn_ref.shape[1])).astype(BF16)
    nt[EDGE:2 * EDGE, :] = newest
    tail(0, 0)[1].wait_recv()
    for c in new_copies:
        c.wait()

    def new_conv(w, start, width):
        pre = rounded(jnp.dot(nt[...], w, preferred_element_type=F32))
        start = pl.multiple_of(start, LANES)
        acc = cb_ref[:, pl.ds(start, width)]
        w = cw_ref[:, pl.ds(start, width)]
        for o in range(taps):
            at = EDGE - taps + 1 + o
            acc = acc + w[o:o + 1] * pre[at:at + 1]
        return rounded(silu_twice(acc))

    skip = lax.rem(j * gl, PAIR)
    new_wx = wxs[steps - 1, :, pl.ds(pl.multiple_of(skip * gcols, LANES), hl * p_size)]
    new_wb = wbs[steps - 1, :, pl.ds(pl.multiple_of(skip * n_size, LANES), gl * n_size)]
    new_values = new_conv(new_wx, vcol, hl * p_size)
    new_keys = new_conv(new_wb, inner + gcol, gl * n_size)
    new_query = new_conv(wcn[...], inner + keys_all + gcol, gl * n_size)
    gate = rounded(jnp.dot(newest, wzn[...], preferred_element_type=F32)[0:1])
    new_raw = rounded(lax.dot_general(
        newest, wdts[...], (((1,), (1,)), ((), ())), preferred_element_type=F32)[0:1])
    new_steps = softplus(new_raw + dtb_ref[...])
    head_s[...] = jnp.zeros_like(head_s)
    head_s[0:1, :] = new_steps
    head_s[1:2, :] = jnp.exp(-jnp.exp(alog_ref[...]) * new_steps)
    head_s[2:3, :] = dskip_ref[...]
    hrow = lax.broadcasted_iota(jnp.int32, (heads, hl * p_size), 0)
    hcol = lax.broadcasted_iota(jnp.int32, (heads, hl * p_size), 1)
    first = j * hl
    onehot = ((hcol >= (hrow - first) * p_size) & (hcol < (hrow - first + 1) * p_size)).astype(F32)
    spread_rows = jnp.dot(head_s[...], onehot, precision=lax.Precision.HIGHEST, preferred_element_type=F32)
    step_row, decay_row, skip_row = spread_rows[0:1], spread_rows[1:2], spread_rows[2:3]

    @pl.when(near)
    def _():
        for s in range(1, steps - 2):
            pass_on(s)
    for s in range(steps - 2, steps):
        pass_on(s)
    def sent(s):
        for gp in range(PAIR):
            a_copy(s, gp).wait_send()
            pl.when(far)(b_copy(s, gp).wait_send)
            here, remote, _ = state_copy(s, gp)
            pl.when(jnp.logical_not(far) & jnp.logical_not(here))(remote.wait_send)

    @pl.when(i != sp - 1)
    def _():
        for r in range(spt):
            halo(r).wait_send()

    @pl.when(i == sp - 1)
    def _():
        for r in range(spt):
            for q in range(tp):
                here, remote, _ = tail(r, q)
                pl.when(jnp.logical_not(here))(remote.wait_send)

    for k in range(sp):
        pl.when(i != k)(tot(k).wait_send)
    for s in range(steps - 1):
        sent(s)
    for g in range(gl):
        for k in range(pairs + 1):
            pltpu.make_async_remote_copy(
                src_ref=st_out.at[0, 0], dst_ref=st_in.at[k, g], send_sem=st_send.at[0, 0],
                recv_sem=st_recv.at[k, g], device_id={"sp": after, "tp": j}, device_id_type=MESH).wait_recv()
        query = new_query[:, g * n_size:(g + 1) * n_size]
        key = new_keys[:, g * n_size:(g + 1) * n_size]
        query_rows = jnp.broadcast_to(query, (EDGE, n_size)).astype(BF16)
        helds = []
        for r in range(ratio):
            h = g * ratio + r
            acc = jnp.zeros((p_size, n_size), F32)
            for k in range(pairs + 1):
                acc += st_in[k, g, r * p_size:(r + 1) * p_size, :].astype(F32)
            top = acc.astype(BF16)
            state_ref[0, h] = top
            held = jnp.zeros((EDGE, p_size), F32)
            rest = acc
            for _ in range(3):
                term = rest.astype(BF16)
                held += lax.dot_general(query_rows, term, (((1,), (1,)), ((), ())), preferred_element_type=F32)
                rest = rest - term.astype(F32)
            helds.append(held[0:1])
        span = slice(g * gcols, (g + 1) * gcols)
        held_row = jnp.concatenate(helds, axis=1)
        inner_prod = jnp.sum(query * key, axis=1, keepdims=True)
        value_row = new_values[:, span]
        out = (decay_row[:, span] * held_row + (step_row[:, span] * inner_prod) * value_row
               + skip_row[:, span] * value_row)
        gated = out * silu(gate[:, span])
        ms = jnp.sum(gated * gated, axis=1, keepdims=True) / gcols
        normed = gated * lax.rsqrt(ms + EPS)
        for r in range(ratio):
            h = g * ratio + r
            read_s[h:h + 1, :] = normed[:, r * p_size:(r + 1) * p_size] * ng_ref[h:h + 1, :]
    read_ref[0] = read_s[...].astype(BF16)

    sent(steps - 1)


def hand_over(state_in, read_in, state_out, read_out):
    state_out[...] = state_in[...]
    read_out[...] = read_in[...]


def per_device(
    dims, x_in, x_new, w_x, w_b, w_c, w_dt, w_z, conv_w, conv_b, dt_bias, a_log, d_skip, norm_g
):
    sp, tp, heads, groups, n_size, p_size, ratio, taps = dims
    spt, length, width = x_in.shape
    hl, gl = heads // tp, groups // tp
    assert x_new.shape[0] == 1 and sp == spt * tp and spt == 2 and sp % 4 == 0 and gl <= PAIR
    steps, gcols = groups // PAIR, ratio * p_size
    tiles = PAIR * (gcols + n_size) // LANES
    any_spec = pl.BlockSpec(memory_space=pl.ANY)
    vmem = pl.BlockSpec(memory_space=pltpu.VMEM)
    dma = pltpu.SemaphoreType.DMA
    results = pl.pallas_call(
        functools.partial(kernel, dims),
        out_shape=(
            jax.ShapeDtypeStruct((1, hl, p_size, n_size), BF16),
            jax.ShapeDtypeStruct((1, hl, p_size), BF16),
        ),
        in_specs=[any_spec, vmem] + [any_spec] * 7 + [vmem] * 4,
        out_specs=(vmem, vmem),
        scratch_shapes=[
            pltpu.VMEM((spt * length + EDGE, width), BF16),
            pltpu.VMEM((steps, width, PAIR * gcols), BF16),
            pltpu.VMEM((steps, width, PAIR * n_size), BF16),
            pltpu.VMEM((heads, width), BF16),
            pltpu.VMEM((width, gl * n_size), BF16),
            pltpu.VMEM((width, hl * p_size), BF16),
            pltpu.VMEM((2 * EDGE, width), BF16),
            pltpu.VMEM((tiles, SENT + length, LANES), F32),
            pltpu.VMEM((tiles, SENT + length, LANES), F32),
            pltpu.VMEM((tiles, SENT + length, LANES), F32),
            pltpu.VMEM((tiles, SENT + length, LANES), F32),
            pltpu.VMEM((spt, length, LANES), F32),
            pltpu.VMEM((length, length), BF16),
            pltpu.VMEM((8, LANES), F32),
            pltpu.VMEM((spt, PAIR, length, n_size), BF16),
            pltpu.VMEM((spt, PAIR, gcols, length), BF16),
            pltpu.VMEM((spt, heads, length), F32),
            pltpu.VMEM((8, LANES), F32),
            pltpu.VMEM((sp, 8, LANES), F32),
            pltpu.VMEM((2, heads, LANES), F32),
            pltpu.VMEM((steps, PAIR, gcols, n_size), BF16),
            pltpu.VMEM((steps, PAIR, gcols, n_size), BF16),
            pltpu.VMEM((steps, PAIR, gcols, n_size), F32),
            pltpu.VMEM((steps, PAIR, gcols, n_size), BF16),
            pltpu.VMEM((steps, PAIR, gcols, n_size), BF16),
            pltpu.VMEM((sp // 4 + 1, gl, gcols, n_size), BF16),
            pltpu.VMEM((8, heads), F32),
            pltpu.VMEM((hl, p_size), F32),
            pltpu.VMEM(conv_w.shape, F32),
            pltpu.VMEM((1, conv_w.shape[1]), F32),
            dma((spt,)), dma, dma((steps, 2)), dma((2,)), dma((2,)), dma((spt,)), dma((spt,)),
            dma((spt, tp)), dma((1,)), dma((sp,)), dma((sp,)), dma((steps, PAIR)), dma((steps, PAIR)),
            dma((steps, PAIR)), dma((steps, PAIR)), dma((steps, PAIR)), dma((sp // 4 + 1, gl)),
        ],
        compiler_params=pltpu.CompilerParams(
            collective_id=0, has_side_effects=True, vmem_limit_bytes=60 * 1024 * 1024
        ),
    )(
        x_in, x_new, w_x, w_b, w_c, w_dt.T, w_z, conv_w, conv_b.reshape(1, -1),
        dt_bias.reshape(1, -1), a_log.reshape(1, -1), d_skip.reshape(1, -1), norm_g,
    )
    return pl.pallas_call(
        hand_over,
        out_shape=tuple(jax.ShapeDtypeStruct(r.shape, r.dtype) for r in results),
        in_specs=[vmem, vmem],
        out_specs=(vmem, vmem),
        compiler_params=pltpu.CompilerParams(vmem_limit_bytes=4 * 1024 * 1024),
    )(*results)


def solution(mesh):
    sp, tp = mesh.shape["sp"], mesh.shape["tp"]

    def step(x_in, x_new, w_x, w_b, w_c, w_dt, w_z, conv_w, conv_b, dt_bias, a_log, d_skip, norm_g):
        heads, p_size = w_dt.shape[1], norm_g.shape[1]
        keys_all = w_b.shape[1]
        n_size = LANES
        groups = keys_all // n_size
        dims = (sp, tp, heads, groups, n_size, p_size, heads // groups, conv_w.shape[0])
        return per_device(
            dims, x_in, x_new, w_x, w_b, w_c, w_dt, w_z, conv_w, conv_b, dt_bias, a_log, d_skip, norm_g)

    return jax.shard_map(
        step,
        mesh=mesh,
        in_specs=(
            P("tp", "sp", None), P("sp", None), P(), P(), P(), P(), P(None, "tp"),
            P(), P(), P(), P(), P(), P("tp", None),
        ),
        out_specs=(P("sp", "tp", None, None), P("sp", "tp", None)),
        check_vma=False,
    )
```

```python
import functools

import jax
import jax.numpy as jnp
from jax import lax
from jax.experimental import pallas as pl
from jax.experimental.pallas import tpu as pltpu
from jax.sharding import PartitionSpec as P

MESH = pl.DeviceIdType.MESH
F32 = jnp.float32
BF16 = jnp.bfloat16
EPS = 1e-05
EDGE = 16
SENT = 8
PAIR = 2
LANES = 128


def silu(x):
    half = 0.5 * x
    return half + half * jnp.tanh(half)


def silu_twice(half):
    return half + half * jnp.tanh(half)


def softplus(x):
    return jnp.maximum(x, 0.0) + jnp.log1p(jnp.exp(-jnp.abs(x)))


def rounded(x):
    return x.astype(BF16).astype(F32)


def kernel(
    dims,
    x_ref, xn_ref, wx_ref, wb_ref, wc_ref, wdt_ref, wz_ref,
    cw_hbm, cb_hbm, dtb_ref, alog_ref, dskip_ref, ng_ref,
    state_ref, read_ref,
    xs, wxs, wbs, wdts, wcn, wzn, nt, pre_s0, pre_s1, pre_o0, pre_o1, pre_o2, padded, later, rows, keys, scaled,
    wt, tot_out, tot_in, fcol, a_out, a_in, mine, b_in, st_out, st_in, head_s, read_s, cw_ref, cb_ref,
    x_sem, wdt_sem, w_sem, new_sem, conv_sem, halo_send, halo_recv, tail_send, tail_recv,
    tot_send, tot_recv, a_send, a_recv, b_send, b_recv, st_send, st_recv,
):
    sp, tp, heads, groups, n_size, p_size, ratio, taps = dims
    i, j = lax.axis_index("sp"), lax.axis_index("tp")
    spt, length, _ = x_ref.shape
    hl, gl = heads // tp, groups // tp
    inner, keys_all = heads * p_size, groups * n_size
    gcols = ratio * p_size
    steps = groups // PAIR
    home = i // spt
    pres = ((pre_s0, pre_s1), (pre_o0, pre_o1, pre_o2))
    member, m = lax.rem(i, 2), i // 2
    direct = m // 2 == j // 2
    near = jnp.logical_not(direct) & ((j > m) == (lax.rem(m, 2) == 1))
    far = jnp.logical_not(direct) & jnp.logical_not(near)
    partner, sibling = i + 1 - 2 * member, i + 2 - 4 * lax.rem(m, 2)
    pairs = sp // 4
    after = lax.rem(i + 1, sp)
    starts = (0, length + EDGE)
    seqs = (1 - member, member)
    width_v, width_k, width_h = PAIR * gcols, PAIR * n_size, PAIR * ratio
    vtiles, ktiles = width_v // LANES, width_k // LANES
    tiles_group = gcols // LANES
    heads_tile = LANES // p_size

    def place(s):
        return lax.rem(s + 1 + (j * gl) // PAIR, steps)

    x_copies = [
        pltpu.make_async_copy(x_ref.at[seqs[r]], xs.at[pl.ds(starts[r], length)], x_sem.at[r])
        for r in range(spt)
    ]
    wdt_copy = pltpu.make_async_copy(wdt_ref, wdts, wdt_sem)

    def w_copies(s):
        at = place(s)
        return (
            pltpu.make_async_copy(
                wx_ref.at[:, pl.ds(pl.multiple_of(at * width_v, LANES), width_v)], wxs.at[s], w_sem.at[s, 0]),
            pltpu.make_async_copy(
                wb_ref.at[:, pl.ds(pl.multiple_of(at * width_k, LANES), width_k)], wbs.at[s], w_sem.at[s, 1]),
        )

    vcol = pl.multiple_of(j * (hl * p_size), LANES)
    gcol = pl.multiple_of(j * (gl * n_size), LANES)
    new_copies = [
        pltpu.make_async_copy(wc_ref.at[:, pl.ds(gcol, gl * n_size)], wcn, new_sem.at[0]),
        pltpu.make_async_copy(wz_ref, wzn, new_sem.at[1]),
    ]
    conv_copies = [
        pltpu.make_async_copy(cw_hbm, cw_ref, conv_sem.at[0]),
        pltpu.make_async_copy(cb_hbm, cb_ref, conv_sem.at[1]),
    ]
    for c in x_copies:
        c.start()
    wdt_copy.start()

    barrier = pltpu.get_barrier_semaphore()
    for k in range(sp):
        @pl.when(i != k)
        def _():
            pl.semaphore_signal(barrier, inc=1, device_id={"sp": k, "tp": j}, device_id_type=MESH)

        @pl.when(home != j)
        def _():
            pl.semaphore_signal(barrier, inc=1, device_id={"sp": k, "tp": home}, device_id_type=MESH)
    for c in w_copies(0):
        c.start()
    for c in conv_copies:
        c.start()

    nt[0:EDGE - SENT, :] = jnp.zeros((EDGE - SENT, nt.shape[1]), BF16)
    padded[...] = jnp.zeros_like(padded)
    rows[...] = jnp.zeros_like(rows)
    for r in range(spt):
        rows[0:1, r * heads:(r + 1) * heads] = -jnp.exp(alog_ref[...])
        rows[1:2, r * heads:(r + 1) * heads] = dtb_ref[...]

    @pl.when(i == 0)
    def _():
        xs[length:length + EDGE, :] = jnp.zeros((EDGE, xs.shape[1]), BF16)

    before = lax.broadcasted_iota(jnp.int32, (length, length), 0)
    column_at = lax.broadcasted_iota(jnp.int32, (length, length), 1)
    later[...] = (before > column_at).astype(F32).astype(BF16)

    def column(row):
        return jnp.broadcast_to(row, (LANES, LANES)).T

    for c in x_copies:
        c.wait()
    pl.semaphore_wait(barrier, sp - 1 + spt * (tp - 1))

    def halo(r):
        return pltpu.make_async_remote_copy(
            src_ref=xs.at[pl.ds(starts[r] + length - SENT, SENT)],
            dst_ref=xs.at[pl.ds(length + SENT * (1 - r), SENT)],
            send_sem=halo_send.at[r], recv_sem=halo_recv.at[1 - r],
            device_id={"sp": after, "tp": j}, device_id_type=MESH)

    def tail(r, q):
        src = xs.at[pl.ds(starts[r] + length - SENT, SENT)]
        dst = nt.at[pl.ds(EDGE - SENT, SENT)]
        target = spt * j + seqs[r]
        return (target == i) & (q == j), pltpu.make_async_remote_copy(
            src_ref=src, dst_ref=dst, send_sem=tail_send.at[r, q], recv_sem=tail_recv.at[0],
            device_id={"sp": target, "tp": q}, device_id_type=MESH
        ), pltpu.make_async_copy(src, dst, tail_recv.at[0])

    @pl.when(i != sp - 1)
    def _():
        for r in range(spt):
            halo(r).start()

    @pl.when(i == sp - 1)
    def _():
        for r in range(spt):
            for q in range(tp):
                here, remote, local = tail(r, q)
                pl.when(jnp.logical_not(here))(remote.start)
                pl.when(here)(local.start)

    wdt_copy.wait()
    for r in range(spt):
        raw = lax.dot_general(
            xs[starts[r]:starts[r] + length, :], wdts[...], (((1,), (1,)), ((), ())), preferred_element_type=F32)
        padded[r, :, 0:heads] = rounded(raw)

    def tot(k):
        return pltpu.make_async_remote_copy(
            src_ref=tot_out, dst_ref=tot_in.at[i], send_sem=tot_send.at[k], recv_sem=tot_recv.at[i],
            device_id={"sp": k, "tp": j}, device_id_type=MESH)

    def decays():
        turned = jnp.concatenate([padded[r].T[0:heads] for r in range(spt)], axis=0)
        rates = column(rows[0:1, :])[0:spt * heads, 0:1]
        biases = column(rows[1:2, :])[0:spt * heads, 0:1]
        sizes = softplus(turned + biases)
        parts, left = [], sizes
        for _ in range(3):
            parts.append(left.astype(BF16))
            left = left - parts[-1].astype(F32)
        sums = jnp.dot(jnp.concatenate(parts, axis=0), later[...], preferred_element_type=F32)
        rest = sum(sums[k * spt * heads:(k + 1) * spt * heads] for k in range(3))
        weights = jnp.exp(rates * rest) * sizes
        for r in range(spt):
            wt[r] = weights[r * heads:(r + 1) * heads]
        total = jnp.broadcast_to(rest[:, 0:1] + sizes[:, 0:1], (spt * heads, LANES))
        given, kept = total[0:heads], total[heads:2 * heads]
        tots = jnp.concatenate([
            jnp.where(member == 0, kept, given), jnp.where(member == 0, given, kept),
            jnp.zeros((LANES - spt * heads, LANES), F32)], axis=0)
        tot_out[...] = tots.T[0:8]

    def factors():
        for k in range(sp):
            @pl.when(i != k)
            def _():
                pltpu.make_async_remote_copy(
                    src_ref=tot_out, dst_ref=tot_in.at[k], send_sem=tot_send.at[k], recv_sem=tot_recv.at[k],
                    device_id={"sp": k, "tp": j}, device_id_type=MESH).wait_recv()
        for at, who in enumerate((i, partner)):
            beyond = jnp.zeros((1, LANES), F32)
            for k in range(sp):
                beyond = beyond + jnp.where(k > who, tot_in[k, 0:1, :], 0.0)
            both = column(jnp.exp(rows[0:1, :] * beyond))
            fcol[at] = jnp.where(member == 0, both[0:heads], both[heads:2 * heads])

    def a_copy(s, gp):
        return pltpu.make_async_remote_copy(
            src_ref=a_out.at[s, gp], dst_ref=a_in.at[s, gp], send_sem=a_send.at[s, gp], recv_sem=a_recv.at[s, gp],
            device_id={"sp": partner, "tp": j}, device_id_type=MESH)

    def b_copy(s, gp):
        return pltpu.make_async_remote_copy(
            src_ref=st_out.at[s, gp], dst_ref=b_in.at[s, gp], send_sem=b_send.at[s, gp], recv_sem=b_recv.at[s, gp],
            device_id={"sp": sibling, "tp": j}, device_id_type=MESH)

    slot = jnp.where(direct & (lax.rem(m, 2) == 1), pairs, m // 2)

    def state_copy(s, gp):
        g = place(s) * PAIR + gp
        q = g // gl
        src, dst = st_out.at[s, gp], st_in.at[slot, lax.rem(g, gl)]
        sem = st_recv.at[slot, lax.rem(g, gl)]
        return (m == j) & (q == j), pltpu.make_async_remote_copy(
            src_ref=src, dst_ref=dst, send_sem=st_send.at[s, gp], recv_sem=sem,
            device_id={"sp": spt * j + member, "tp": q}, device_id_type=MESH
        ), pltpu.make_async_copy(src, dst, sem)

    def pass_on(joined, s, gp):
        at = pl.multiple_of(place(s) * width_h, width_h)

        def add(gp, *more):
            scales = [fcol[k, pl.ds(at, width_h), :] for k in range(2)]
            for r in range(ratio):
                h, span = gp * ratio + r, slice(r * p_size, (r + 1) * p_size)
                total = scales[0][h:h + 1] * mine[s, gp, span, :]
                total += scales[1][h:h + 1] * a_in[s, gp, span, :].astype(F32)
                for ref in more:
                    total += ref[s, gp, span, :].astype(F32)
                st_out[s, gp, span, :] = total.astype(BF16)

        a_copy(s, gp).wait_recv()
        if joined:
            b_copy(s, gp).wait_recv()
            add(gp, b_in)
        else:
            add(gp)
            pl.when(far)(b_copy(s, gp).start)

        @pl.when(jnp.logical_not(far))
        def _():
            here, remote, local = state_copy(s, gp)
            pl.when(jnp.logical_not(here))(remote.start)
            pl.when(here)(local.start)

    def project(s, first, count, w, base, tiles, keep):
        cuts = [0, count] if tiles > 2 else [0, count // 2 // EDGE * EDGE, count]
        out = jnp.concatenate([
            jnp.dot(xs[first + lo:first + hi, :], w[s], preferred_element_type=F32)
            for lo, hi in zip(cuts, cuts[1:])], axis=0)
        for c in range(tiles):
            keep(base + c, out[:, c * LANES:(c + 1) * LANES])

    def given_alone(s):
        def keep(c, v):
            pres[0][s % 2][c, SENT:SENT + length, :] = v
        return s, 0, length, keep

    def given_with_edges(s):
        def keep(c, v):
            pres[0][s % 2][c, SENT:SENT + length, :] = v[0:length]
            pres[0][s % 2][c, 0:SENT, :] = v[length:length + SENT]
            pres[1][s % 3][c, 0:SENT, :] = v[length + SENT:length + EDGE]
        return s, 0, length + EDGE, keep

    def kept_with_edges(s):
        def keep(c, v):
            pres[0][s % 2][c, 0:SENT, :] = v[0:SENT]
            pres[1][s % 3][c, :, :] = v[SENT:EDGE + length]
        return s, length, length + EDGE, keep

    def kept_alone(s):
        def keep(c, v):
            pres[1][s % 3][c, SENT:SENT + length, :] = v
        return s, length + EDGE, length, keep

    def values_of(job):
        s, first, count, keep = job
        project(s, first, count, wxs, 0, vtiles, keep)

    def keys_of(job):
        s, first, count, keep = job
        project(s, first, count, wbs, vtiles, ktiles, keep)

    def contract(s, r, b):
        place_s = place(s)
        pre = pres[r][s % len(pres[r])]

        def conv(c):
            if c < vtiles:
                at = pl.multiple_of(place_s * width_v + c * LANES, LANES)
            else:
                at = pl.multiple_of(inner + place_s * width_k + (c - vtiles) * LANES, LANES)
            acc = cb_ref[:, pl.ds(at, LANES)]
            w = cw_ref[:, pl.ds(at, LANES)]
            for o in range(taps):
                acc = acc + w[o:o + 1] * pre[c, pl.ds(SENT - taps + 1 + o, length), :]
            return silu_twice(acc).astype(BF16)

        weights = wt[r, pl.ds(pl.multiple_of(place_s * width_h, width_h), width_h), :]
        for gp in range(PAIR):
            keys[b, gp] = conv(vtiles + gp)
            for c in range(gp * tiles_group, (gp + 1) * tiles_group):
                turned = conv(c).T
                for k in range(heads_tile):
                    h = c * heads_tile + k
                    part = turned[k * p_size:(k + 1) * p_size].astype(F32)
                    scaled[b, gp, (h - gp * ratio) * p_size:(h - gp * ratio + 1) * p_size] = (
                        weights[h:h + 1] * part).astype(BF16)

    def combine(s, r, b):
        outs = [jnp.dot(scaled[b, gp], keys[b, gp], preferred_element_type=F32) for gp in range(PAIR)]
        for gp in range(PAIR):
            if r == 0:
                a_out[s, gp] = outs[gp].astype(BF16)
            else:
                mine[s, gp] = outs[gp]
        if r == 0:
            for gp in range(PAIR):
                a_copy(s, gp).start()

    def w_wait(s):
        for c in w_copies(s):
            c.wait()

    w_wait(0)
    for c in w_copies(1):
        c.start()
    values_of(given_alone(0))
    decays()
    keys_of(given_alone(0))

    tot_in[i] = tot_out[...]
    for k in range(sp):
        pl.when(i != k)(tot(k).start)

    @pl.when(i != 0)
    def _():
        for r in range(spt):
            halo(r).wait_recv()
    for s in range(2, steps):
        for c in w_copies(s):
            c.start()
    for c in new_copies:
        c.start()
    for c in conv_copies:
        c.wait()
    cw_ref[...] = 0.5 * cw_ref[...]
    cb_ref[...] = 0.5 * cb_ref[...]

    def block(job, turn):
        if turn is None:
            values_of(job)
            keys_of(job)
            return
        s, r, b = turn
        values_of(job)
        keys_of(job)
        contract(s, r, b)
        combine(s, r, b)

    def others(*pieces):
        for s, gp in pieces:
            pl.when(jnp.logical_not(near))(functools.partial(pass_on, False, s, gp))

    def nears(*pieces):
        for s, gp in pieces:
            pl.when(near)(functools.partial(pass_on, True, s, gp))

    order = [(0, 0), (0, 1)]
    for s in range(1, steps):
        at = len(order) - 1 if s > 1 else len(order)
        order.insert(at, (s, 0))
        order.append((s, 1))
    pieces = [(s, gp) for s in range(steps) for gp in range(PAIR)]
    for k in range(1, len(order)):
        s, r = order[k]
        if r == 0:
            w_wait(s)
        job = kept_with_edges(0) if k == 1 else given_with_edges(s) if r == 0 else kept_alone(s)
        block(job, order[k - 1] + ((k - 1) % 2,))
        if k == 3:
            factors()
        if k >= 3:
            others(pieces[k - 3])
        if k == len(order) - 2:
            nears(*pieces[:2])
        if k == len(order) - 1:
            nears(pieces[2])
    s, r = order[-1]
    contract(s, r, (len(order) - 1) % 2)
    combine(s, r, (len(order) - 1) % 2)
    others(*pieces[len(order) - 3:])

    newest = jnp.broadcast_to(xn_ref[...].astype(F32), (EDGE, xn_ref.shape[1])).astype(BF16)
    nt[EDGE:2 * EDGE, :] = newest
    tail(0, 0)[1].wait_recv()
    for c in new_copies:
        c.wait()

    def new_conv(w, start, width):
        pre = rounded(jnp.dot(nt[...], w, preferred_element_type=F32))
        start = pl.multiple_of(start, LANES)
        acc = cb_ref[:, pl.ds(start, width)]
        w = cw_ref[:, pl.ds(start, width)]
        for o in range(taps):
            at = EDGE - taps + 1 + o
            acc = acc + w[o:o + 1] * pre[at:at + 1]
        return rounded(silu_twice(acc))

    skip = lax.rem(j * gl, PAIR)
    new_wx = wxs[steps - 1, :, pl.ds(pl.multiple_of(skip * gcols, LANES), hl * p_size)]
    new_wb = wbs[steps - 1, :, pl.ds(pl.multiple_of(skip * n_size, LANES), gl * n_size)]
    new_values = new_conv(new_wx, vcol, hl * p_size)
    new_keys = new_conv(new_wb, inner + gcol, gl * n_size)
    new_query = new_conv(wcn[...], inner + keys_all + gcol, gl * n_size)
    gate = rounded(jnp.dot(newest, wzn[...], preferred_element_type=F32)[0:1])
    new_raw = rounded(lax.dot_general(
        newest, wdts[...], (((1,), (1,)), ((), ())), preferred_element_type=F32)[0:1])
    new_steps = softplus(new_raw + dtb_ref[...])
    head_s[...] = jnp.zeros_like(head_s)
    head_s[0:1, :] = new_steps
    head_s[1:2, :] = jnp.exp(-jnp.exp(alog_ref[...]) * new_steps)
    head_s[2:3, :] = dskip_ref[...]
    hrow = lax.broadcasted_iota(jnp.int32, (heads, hl * p_size), 0)
    hcol = lax.broadcasted_iota(jnp.int32, (heads, hl * p_size), 1)
    first = j * hl
    onehot = ((hcol >= (hrow - first) * p_size) & (hcol < (hrow - first + 1) * p_size)).astype(F32)
    spread_rows = jnp.dot(head_s[...], onehot, precision=lax.Precision.HIGHEST, preferred_element_type=F32)
    step_row, decay_row, skip_row = spread_rows[0:1], spread_rows[1:2], spread_rows[2:3]

    nears(*pieces[3:])

    def sent(s):
        for gp in range(PAIR):
            a_copy(s, gp).wait_send()
            pl.when(far)(b_copy(s, gp).wait_send)
            here, remote, _ = state_copy(s, gp)
            pl.when(jnp.logical_not(far) & jnp.logical_not(here))(remote.wait_send)

    @pl.when(i != sp - 1)
    def _():
        for r in range(spt):
            halo(r).wait_send()

    @pl.when(i == sp - 1)
    def _():
        for r in range(spt):
            for q in range(tp):
                here, remote, _ = tail(r, q)
                pl.when(jnp.logical_not(here))(remote.wait_send)

    for k in range(sp):
        pl.when(i != k)(tot(k).wait_send)
    for s in range(steps - 1):
        sent(s)
    for g in range(gl):
        for k in range(pairs + 1):
            pltpu.make_async_remote_copy(
                src_ref=st_out.at[0, 0], dst_ref=st_in.at[k, g], send_sem=st_send.at[0, 0],
                recv_sem=st_recv.at[k, g], device_id={"sp": after, "tp": j}, device_id_type=MESH).wait_recv()
        query = new_query[:, g * n_size:(g + 1) * n_size]
        key = new_keys[:, g * n_size:(g + 1) * n_size]
        query_rows = jnp.broadcast_to(query, (EDGE, n_size)).astype(BF16)
        helds = []
        for r in range(ratio):
            h = g * ratio + r
            acc = jnp.zeros((p_size, n_size), F32)
            for k in range(pairs + 1):
                acc += st_in[k, g, r * p_size:(r + 1) * p_size, :].astype(F32)
            top = acc.astype(BF16)
            state_ref[0, h] = top
            held = jnp.zeros((EDGE, p_size), F32)
            rest = acc
            for _ in range(3):
                term = rest.astype(BF16)
                held += lax.dot_general(query_rows, term, (((1,), (1,)), ((), ())), preferred_element_type=F32)
                rest = rest - term.astype(F32)
            helds.append(held[0:1])
        span = slice(g * gcols, (g + 1) * gcols)
        held_row = jnp.concatenate(helds, axis=1)
        inner_prod = jnp.sum(query * key, axis=1, keepdims=True)
        value_row = new_values[:, span]
        out = (decay_row[:, span] * held_row + (step_row[:, span] * inner_prod) * value_row
               + skip_row[:, span] * value_row)
        gated = out * silu(gate[:, span])
        ms = jnp.sum(gated * gated, axis=1, keepdims=True) / gcols
        normed = gated * lax.rsqrt(ms + EPS)
        for r in range(ratio):
            h = g * ratio + r
            read_s[h:h + 1, :] = normed[:, r * p_size:(r + 1) * p_size] * ng_ref[h:h + 1, :]
    read_ref[0] = read_s[...].astype(BF16)

    sent(steps - 1)


def hand_over(state_in, read_in, state_out, read_out):
    state_out[...] = state_in[...]
    read_out[...] = read_in[...]


def per_device(
    dims, x_in, x_new, w_x, w_b, w_c, w_dt, w_z, conv_w, conv_b, dt_bias, a_log, d_skip, norm_g
):
    sp, tp, heads, groups, n_size, p_size, ratio, taps = dims
    spt, length, width = x_in.shape
    hl, gl = heads // tp, groups // tp
    assert x_new.shape[0] == 1 and sp == spt * tp and spt == 2 and sp % 4 == 0 and gl <= PAIR
    steps, gcols = groups // PAIR, ratio * p_size
    tiles = PAIR * (gcols + n_size) // LANES
    any_spec = pl.BlockSpec(memory_space=pl.ANY)
    vmem = pl.BlockSpec(memory_space=pltpu.VMEM)
    dma = pltpu.SemaphoreType.DMA
    results = pl.pallas_call(
        functools.partial(kernel, dims),
        out_shape=(
            pltpu.VMEM((1, hl, p_size, n_size), BF16),
            pltpu.VMEM((1, hl, p_size), BF16),
        ),
        in_specs=[any_spec, vmem] + [any_spec] * 7 + [vmem] * 4,
        out_specs=(vmem, vmem),
        scratch_shapes=[
            pltpu.VMEM((spt * length + EDGE, width), BF16),
            pltpu.VMEM((steps, width, PAIR * gcols), BF16),
            pltpu.VMEM((steps, width, PAIR * n_size), BF16),
            pltpu.VMEM((heads, width), BF16),
            pltpu.VMEM((width, gl * n_size), BF16),
            pltpu.VMEM((width, hl * p_size), BF16),
            pltpu.VMEM((2 * EDGE, width), BF16),
            pltpu.VMEM((tiles, SENT + length, LANES), F32),
            pltpu.VMEM((tiles, SENT + length, LANES), F32),
            pltpu.VMEM((tiles, SENT + length, LANES), F32),
            pltpu.VMEM((tiles, SENT + length, LANES), F32),
            pltpu.VMEM((tiles, SENT + length, LANES), F32),
            pltpu.VMEM((spt, length, LANES), F32),
            pltpu.VMEM((length, length), BF16),
            pltpu.VMEM((8, LANES), F32),
            pltpu.VMEM((spt, PAIR, length, n_size), BF16),
            pltpu.VMEM((spt, PAIR, gcols, length), BF16),
            pltpu.VMEM((spt, heads, length), F32),
            pltpu.VMEM((8, LANES), F32),
            pltpu.VMEM((sp, 8, LANES), F32),
            pltpu.VMEM((2, heads, LANES), F32),
            pltpu.VMEM((steps, PAIR, gcols, n_size), BF16),
            pltpu.VMEM((steps, PAIR, gcols, n_size), BF16),
            pltpu.VMEM((steps, PAIR, gcols, n_size), F32),
            pltpu.VMEM((steps, PAIR, gcols, n_size), BF16),
            pltpu.VMEM((steps, PAIR, gcols, n_size), BF16),
            pltpu.VMEM((sp // 4 + 1, gl, gcols, n_size), BF16),
            pltpu.VMEM((8, heads), F32),
            pltpu.VMEM((hl, p_size), F32),
            pltpu.VMEM(conv_w.shape, F32),
            pltpu.VMEM((1, conv_w.shape[1]), F32),
            dma((spt,)), dma, dma((steps, 2)), dma((2,)), dma((2,)), dma((spt,)), dma((spt,)),
            dma((spt, tp)), dma((1,)), dma((sp,)), dma((sp,)), dma((steps, PAIR)), dma((steps, PAIR)),
            dma((steps, PAIR)), dma((steps, PAIR)), dma((steps, PAIR)), dma((sp // 4 + 1, gl)),
        ],
        compiler_params=pltpu.CompilerParams(
            collective_id=0, has_side_effects=True, vmem_limit_bytes=60 * 1024 * 1024
        ),
    )(
        x_in, x_new, w_x, w_b, w_c, w_dt.T, w_z, conv_w, conv_b.reshape(1, -1),
        dt_bias.reshape(1, -1), a_log.reshape(1, -1), d_skip.reshape(1, -1), norm_g,
    )
    return pl.pallas_call(
        hand_over,
        out_shape=tuple(jax.ShapeDtypeStruct(r.shape, r.dtype) for r in results),
        in_specs=[vmem, vmem],
        out_specs=(vmem, vmem),
        compiler_params=pltpu.CompilerParams(vmem_limit_bytes=4 * 1024 * 1024),
    )(*results)


def solution(mesh):
    sp, tp = mesh.shape["sp"], mesh.shape["tp"]

    def step(x_in, x_new, w_x, w_b, w_c, w_dt, w_z, conv_w, conv_b, dt_bias, a_log, d_skip, norm_g):
        heads, p_size = w_dt.shape[1], norm_g.shape[1]
        keys_all = w_b.shape[1]
        n_size = LANES
        groups = keys_all // n_size
        dims = (sp, tp, heads, groups, n_size, p_size, heads // groups, conv_w.shape[0])
        return per_device(
            dims, x_in, x_new, w_x, w_b, w_c, w_dt, w_z, conv_w, conv_b, dt_bias, a_log, d_skip, norm_g)

    return jax.shard_map(
        step,
        mesh=mesh,
        in_specs=(
            P("tp", "sp", None), P("sp", None), P(), P(), P(), P(), P(None, "tp"),
            P(), P(), P(), P(), P(), P("tp", None),
        ),
        out_specs=(P("sp", "tp", None, None), P("sp", "tp", None)),
        check_vma=False,
    )
```

```python
import functools

import jax
import jax.numpy as jnp
from jax import lax
from jax.experimental import pallas as pl
from jax.experimental.pallas import tpu as pltpu
from jax.sharding import PartitionSpec as P

MESH = pl.DeviceIdType.MESH
F32 = jnp.float32
BF16 = jnp.bfloat16
EPS = 1e-05
EDGE = 16
SENT = 8
HALF = 4
PAIR = 2
LANES = 128


def silu(x):
    half = 0.5 * x
    return half + half * jnp.tanh(half)


def silu_twice(half):
    return half + half * jnp.tanh(half)


def softplus(x):
    return jnp.maximum(x, 0.0) + jnp.log1p(jnp.exp(-jnp.abs(x)))


def rounded(x):
    return x.astype(BF16).astype(F32)


def kernel(
    dims,
    x_ref, xn_ref, wx_ref, wb_ref, wc_ref, wdt_ref, wz_ref,
    cw_hbm, cb_hbm, dtb_ref, alog_ref, dskip_ref, ng_ref,
    state_ref, read_ref,
    xs, wxs, wbs, wdts, wcn, wzn, nt, pre_s0, pre_s1, pre_o0, pre_o1, pre_o2, padded, later, rows, keys, scaled,
    wt, tot_out, tot_in, fcol, a_out, a_in, mine, b_in, st_out, st_in, head_s, read_s, cw_ref, cb_ref, edges,
    x_sem, wdt_sem, w_sem, new_sem, conv_sem, halo_send, halo_recv, tail_send, tail_recv,
    tot_send, tot_recv, a_send, a_recv, b_send, b_recv, st_send, st_recv,
):
    sp, tp, heads, groups, n_size, p_size, ratio, taps = dims
    i, j = lax.axis_index("sp"), lax.axis_index("tp")
    spt, length, _ = x_ref.shape
    hl, gl = heads // tp, groups // tp
    inner, keys_all = heads * p_size, groups * n_size
    gcols = ratio * p_size
    steps = groups // PAIR
    home = i // spt
    pres = ((pre_s0, pre_s1), (pre_o0, pre_o1, pre_o2))
    member, m = lax.rem(i, 2), i // 2
    direct = m // 2 == j // 2
    near = jnp.logical_not(direct) & ((j > m) == (lax.rem(m, 2) == 1))
    far = jnp.logical_not(direct) & jnp.logical_not(near)
    partner, sibling = i + 1 - 2 * member, i + 2 - 4 * lax.rem(m, 2)
    pairs = sp // 4
    after = lax.rem(i + 1, sp)
    starts = (0, length + EDGE)
    seqs = (1 - member, member)
    width_v, width_k, width_h = PAIR * gcols, PAIR * n_size, PAIR * ratio
    vtiles, ktiles = width_v // LANES, width_k // LANES
    tiles_group = gcols // LANES
    heads_tile = LANES // p_size

    def place(s):
        return lax.rem(s + 1 + steps // 2 + (j * gl) // PAIR, steps)

    x_copies = [
        pltpu.make_async_copy(x_ref.at[seqs[r]], xs.at[pl.ds(starts[r], length)], x_sem.at[r])
        for r in range(spt)
    ]
    wdt_copy = pltpu.make_async_copy(wdt_ref, wdts, wdt_sem)

    def w_copies(s):
        at = place(s)
        return (
            pltpu.make_async_copy(
                wx_ref.at[:, pl.ds(pl.multiple_of(at * width_v, LANES), width_v)], wxs.at[s], w_sem.at[s, 0]),
            pltpu.make_async_copy(
                wb_ref.at[:, pl.ds(pl.multiple_of(at * width_k, LANES), width_k)], wbs.at[s], w_sem.at[s, 1]),
        )

    vcol = pl.multiple_of(j * (hl * p_size), LANES)
    gcol = pl.multiple_of(j * (gl * n_size), LANES)
    new_copies = [
        pltpu.make_async_copy(wc_ref.at[:, pl.ds(gcol, gl * n_size)], wcn, new_sem.at[0]),
        pltpu.make_async_copy(wz_ref, wzn, new_sem.at[1]),
    ]
    conv_copies = [
        pltpu.make_async_copy(cw_hbm, cw_ref, conv_sem.at[0]),
        pltpu.make_async_copy(cb_hbm, cb_ref, conv_sem.at[1]),
    ]
    x_copies[0].start()
    wdt_copy.start()
    x_copies[1].start()

    barrier = pltpu.get_barrier_semaphore()
    for k in range(sp):
        @pl.when(i != k)
        def _():
            pl.semaphore_signal(barrier, inc=1, device_id={"sp": k, "tp": j}, device_id_type=MESH)

        @pl.when(home != j)
        def _():
            pl.semaphore_signal(barrier, inc=1, device_id={"sp": k, "tp": home}, device_id_type=MESH)
    for c in w_copies(0):
        c.start(priority=1)
    for c in conv_copies:
        c.start()

    nt[0:EDGE - SENT, :] = jnp.zeros((EDGE - SENT, nt.shape[1]), BF16)
    padded[...] = jnp.zeros_like(padded)
    rows[...] = jnp.zeros_like(rows)
    for r in range(spt):
        rows[0:1, r * heads:(r + 1) * heads] = -jnp.exp(alog_ref[...])
        rows[1:2, r * heads:(r + 1) * heads] = dtb_ref[...]

    xs[length + SENT:length + EDGE, :] = jnp.zeros((EDGE - SENT, xs.shape[1]), BF16)

    @pl.when(i == 0)
    def _():
        xs[length:length + SENT, :] = jnp.zeros((SENT, xs.shape[1]), BF16)

    before = lax.broadcasted_iota(jnp.int32, (length, length), 0)
    column_at = lax.broadcasted_iota(jnp.int32, (length, length), 1)
    later[...] = (before > column_at).astype(F32).astype(BF16)

    def column(row):
        return jnp.broadcast_to(row, (LANES, LANES)).T

    def raw_steps(r):
        for lo in range(0, length, length // 2):
            raw = lax.dot_general(
                xs[starts[r] + lo:starts[r] + lo + length // 2, :], wdts[...], (((1,), (1,)), ((), ())),
                preferred_element_type=F32)
            padded[r, lo:lo + length // 2, 0:heads] = rounded(raw)

    x_copies[0].wait()
    wdt_copy.wait()
    raw_steps(0)
    x_copies[1].wait()
    lasts = [xs[starts[r] + length - EDGE:starts[r] + length, :].astype(F32) for r in range(spt)]
    edges[...] = jnp.concatenate([lasts[1][EDGE - HALF:], lasts[0][EDGE - HALF:]], axis=0).astype(BF16)
    pl.semaphore_wait(barrier, sp - 1 + spt * (tp - 1))

    halo = pltpu.make_async_remote_copy(
        src_ref=edges, dst_ref=xs.at[pl.ds(length, SENT)], send_sem=halo_send.at[0], recv_sem=halo_recv.at[0],
        device_id={"sp": after, "tp": j}, device_id_type=MESH)

    def tail(r, q):
        src = xs.at[pl.ds(starts[r] + length - SENT, SENT)]
        dst = nt.at[pl.ds(EDGE - SENT, SENT)]
        target = spt * j + seqs[r]
        return (target == i) & (q == j), pltpu.make_async_remote_copy(
            src_ref=src, dst_ref=dst, send_sem=tail_send.at[r, q], recv_sem=tail_recv.at[0],
            device_id={"sp": target, "tp": q}, device_id_type=MESH
        ), pltpu.make_async_copy(src, dst, tail_recv.at[0])

    pl.when(i != sp - 1)(halo.start)

    @pl.when(i == sp - 1)
    def _():
        for r in range(spt):
            for q in range(tp):
                here, remote, local = tail(r, q)
                pl.when(jnp.logical_not(here))(remote.start)
                pl.when(here)(local.start)

    raw_steps(1)

    def tot(k):
        return pltpu.make_async_remote_copy(
            src_ref=tot_out, dst_ref=tot_in.at[i], send_sem=tot_send.at[k], recv_sem=tot_recv.at[i],
            device_id={"sp": k, "tp": j}, device_id_type=MESH)

    def decays():
        turned = jnp.concatenate([padded[r].T[0:heads] for r in range(spt)], axis=0)
        rates = column(rows[0:1, :])[0:spt * heads, 0:1]
        biases = column(rows[1:2, :])[0:spt * heads, 0:1]
        sizes = softplus(turned + biases)
        parts, left = [], sizes
        for _ in range(3):
            parts.append(left.astype(BF16))
            left = left - parts[-1].astype(F32)
        sums = jnp.dot(jnp.concatenate(parts, axis=0), later[...], preferred_element_type=F32)
        rest = sum(sums[k * spt * heads:(k + 1) * spt * heads] for k in range(3))
        weights = jnp.exp(rates * rest) * sizes
        for r in range(spt):
            wt[r] = weights[r * heads:(r + 1) * heads]
        total = jnp.broadcast_to(rest[:, 0:1] + sizes[:, 0:1], (spt * heads, LANES))
        given, kept = total[0:heads], total[heads:2 * heads]
        tots = jnp.concatenate([
            jnp.where(member == 0, kept, given), jnp.where(member == 0, given, kept),
            jnp.zeros((LANES - spt * heads, LANES), F32)], axis=0)
        tot_out[...] = tots.T[0:8]

    def factors():
        for k in range(sp):
            @pl.when(i != k)
            def _():
                pltpu.make_async_remote_copy(
                    src_ref=tot_out, dst_ref=tot_in.at[k], send_sem=tot_send.at[k], recv_sem=tot_recv.at[k],
                    device_id={"sp": k, "tp": j}, device_id_type=MESH).wait_recv()
        for at, who in enumerate((i, partner)):
            beyond = jnp.zeros((1, LANES), F32)
            for k in range(sp):
                beyond = beyond + jnp.where(k > who, tot_in[k, 0:1, :], 0.0)
            both = column(jnp.exp(rows[0:1, :] * beyond))
            fcol[at] = jnp.where(member == 0, both[0:heads], both[heads:2 * heads])

    def a_copy(s, gp):
        return pltpu.make_async_remote_copy(
            src_ref=a_out.at[s, gp], dst_ref=a_in.at[s, gp], send_sem=a_send.at[s, gp], recv_sem=a_recv.at[s, gp],
            device_id={"sp": partner, "tp": j}, device_id_type=MESH)

    def b_copy(s, gp):
        return pltpu.make_async_remote_copy(
            src_ref=st_out.at[s, gp], dst_ref=b_in.at[s, gp], send_sem=b_send.at[s, gp], recv_sem=b_recv.at[s, gp],
            device_id={"sp": sibling, "tp": j}, device_id_type=MESH)

    slot = jnp.where(direct & (lax.rem(m, 2) == 1), pairs, m // 2)

    def state_copy(s, gp):
        g = place(s) * PAIR + gp
        q = g // gl
        src, dst = st_out.at[s, gp], st_in.at[slot, lax.rem(g, gl)]
        sem = st_recv.at[slot, lax.rem(g, gl)]
        return (m == j) & (q == j), pltpu.make_async_remote_copy(
            src_ref=src, dst_ref=dst, send_sem=st_send.at[s, gp], recv_sem=sem,
            device_id={"sp": spt * j + member, "tp": q}, device_id_type=MESH
        ), pltpu.make_async_copy(src, dst, sem)

    def pass_on(joined, s, gp):
        at = pl.multiple_of(place(s) * width_h, width_h)

        def add(gp, *more):
            scales = [fcol[k, pl.ds(at, width_h), :] for k in range(2)]
            for r in range(ratio):
                h, span = gp * ratio + r, slice(r * p_size, (r + 1) * p_size)
                total = scales[0][h:h + 1] * mine[s, gp, span, :]
                total += scales[1][h:h + 1] * a_in[s, gp, span, :].astype(F32)
                for ref in more:
                    total += ref[s, gp, span, :].astype(F32)
                st_out[s, gp, span, :] = total.astype(BF16)

        a_copy(s, gp).wait_recv()
        if joined:
            b_copy(s, gp).wait_recv()
            add(gp, b_in)
        else:
            add(gp)
            pl.when(far)(b_copy(s, gp).start)

        @pl.when(jnp.logical_not(far))
        def _():
            here, remote, local = state_copy(s, gp)
            pl.when(jnp.logical_not(here))(remote.start)
            pl.when(here)(local.start)

    def project(s, first, count, w, base, tiles, keep):
        cuts = [0, count] if tiles > 2 else [0, count // 2 // EDGE * EDGE, count]
        out = jnp.concatenate([
            jnp.dot(xs[first + lo:first + hi, :], w[s], preferred_element_type=F32)
            for lo, hi in zip(cuts, cuts[1:])], axis=0)
        for c in range(tiles):
            keep(base + c, out[:, c * LANES:(c + 1) * LANES])

    def given_alone(s):
        def keep(c, v):
            pres[0][s % 2][c, SENT:SENT + length, :] = v
        return s, 0, length, keep

    def given_with_edges(s):
        def keep(c, v):
            pres[0][s % 2][c, SENT:SENT + length, :] = v[0:length]
            pres[0][s % 2][c, HALF:SENT, :] = v[length:length + HALF]
            pres[1][s % 3][c, HALF:SENT, :] = v[length + HALF:length + SENT]
        return s, 0, length + EDGE, keep

    def kept_with_edges(s):
        def keep(c, v):
            pres[0][s % 2][c, HALF:SENT, :] = v[0:HALF]
            pres[1][s % 3][c, HALF:SENT, :] = v[HALF:SENT]
            pres[1][s % 3][c, SENT:SENT + length, :] = v[EDGE:EDGE + length]
        return s, length, length + EDGE, keep

    def kept_alone(s):
        def keep(c, v):
            pres[1][s % 3][c, SENT:SENT + length, :] = v
        return s, length + EDGE, length, keep

    def values_of(job):
        s, first, count, keep = job
        project(s, first, count, wxs, 0, vtiles, keep)

    def keys_of(job):
        s, first, count, keep = job
        project(s, first, count, wbs, vtiles, ktiles, keep)

    def contract(s, r, b):
        place_s = place(s)
        pre = pres[r][s % len(pres[r])]

        def conv(c):
            if c < vtiles:
                at = pl.multiple_of(place_s * width_v + c * LANES, LANES)
            else:
                at = pl.multiple_of(inner + place_s * width_k + (c - vtiles) * LANES, LANES)
            acc = cb_ref[:, pl.ds(at, LANES)]
            w = cw_ref[:, pl.ds(at, LANES)]
            for o in range(taps):
                acc = acc + w[o:o + 1] * pre[c, pl.ds(SENT - taps + 1 + o, length), :]
            return silu_twice(acc).astype(BF16)

        weights = wt[r, pl.ds(pl.multiple_of(place_s * width_h, width_h), width_h), :]
        for gp in range(PAIR):
            keys[b, gp] = conv(vtiles + gp)
            for c in range(gp * tiles_group, (gp + 1) * tiles_group):
                turned = conv(c).T
                for k in range(heads_tile):
                    h = c * heads_tile + k
                    part = turned[k * p_size:(k + 1) * p_size].astype(F32)
                    scaled[b, gp, (h - gp * ratio) * p_size:(h - gp * ratio + 1) * p_size] = (
                        weights[h:h + 1] * part).astype(BF16)

    def combine(s, r, b):
        outs = [jnp.dot(scaled[b, gp], keys[b, gp], preferred_element_type=F32) for gp in range(PAIR)]
        for gp in range(PAIR):
            if r == 0:
                a_out[s, gp] = outs[gp].astype(BF16)
            else:
                mine[s, gp] = outs[gp]
        if r == 0:
            for gp in range(PAIR):
                a_copy(s, gp).start()

    def w_wait(s):
        for c in w_copies(s):
            c.wait()

    w_wait(0)
    for c in w_copies(1):
        c.start()
    values_of(given_alone(0))
    decays()
    keys_of(given_alone(0))

    tot_in[i] = tot_out[...]
    for k in range(sp):
        pl.when(i != k)(tot(k).start)

    pl.when(i != 0)(halo.wait_recv)
    for s in range(2, steps):
        for c in w_copies(s):
            c.start()
    for c in new_copies:
        c.start()
    for c in conv_copies:
        c.wait()
    cw_ref[...] = 0.5 * cw_ref[...]
    cb_ref[...] = 0.5 * cb_ref[...]

    def block(job, turn):
        if turn is None:
            values_of(job)
            keys_of(job)
            return
        s, r, b = turn
        values_of(job)
        keys_of(job)
        contract(s, r, b)
        combine(s, r, b)

    def others(*pieces):
        for s, gp in pieces:
            pl.when(jnp.logical_not(near))(functools.partial(pass_on, False, s, gp))

    def nears(*pieces):
        for s, gp in pieces:
            pl.when(near)(functools.partial(pass_on, True, s, gp))

    order = [(0, 0), (0, 1)]
    for s in range(1, steps):
        at = len(order) - 1 if s > 1 else len(order)
        order.insert(at, (s, 0))
        order.append((s, 1))
    pieces = [(s, gp) for s in range(steps) for gp in range(PAIR)]
    for k in range(1, len(order)):
        s, r = order[k]
        if r == 0:
            w_wait(s)
        job = kept_with_edges(0) if k == 1 else given_with_edges(s) if r == 0 else kept_alone(s)
        block(job, order[k - 1] + ((k - 1) % 2,))
        if k == 3:
            factors()
        if k >= 3:
            others(pieces[k - 3])
        if k == len(order) - 2:
            nears(*pieces[:2])
        if k == len(order) - 1:
            nears(pieces[2])
    others(pieces[len(order) - 3])

    newest = jnp.broadcast_to(xn_ref[...].astype(F32), (EDGE, xn_ref.shape[1])).astype(BF16)
    nt[EDGE:2 * EDGE, :] = newest
    tail(0, 0)[1].wait_recv()
    for c in new_copies:
        c.wait()

    s, r = order[-1]
    contract(s, r, (len(order) - 1) % 2)
    combine(s, r, (len(order) - 1) % 2)

    def new_conv(w, start, width):
        pre = rounded(jnp.dot(nt[...], w, preferred_element_type=F32))
        start = pl.multiple_of(start, LANES)
        acc = cb_ref[:, pl.ds(start, width)]
        w = cw_ref[:, pl.ds(start, width)]
        for o in range(taps):
            at = EDGE - taps + 1 + o
            acc = acc + w[o:o + 1] * pre[at:at + 1]
        return rounded(silu_twice(acc))

    skip = lax.rem(j * gl, PAIR)
    new_wx = wxs[steps // 2 - 1, :, pl.ds(pl.multiple_of(skip * gcols, LANES), hl * p_size)]
    new_wb = wbs[steps // 2 - 1, :, pl.ds(pl.multiple_of(skip * n_size, LANES), gl * n_size)]
    new_values = new_conv(new_wx, vcol, hl * p_size)
    new_keys = new_conv(new_wb, inner + gcol, gl * n_size)
    new_query = new_conv(wcn[...], inner + keys_all + gcol, gl * n_size)
    gate = rounded(jnp.dot(newest, wzn[...], preferred_element_type=F32)[0:1])
    new_raw = rounded(lax.dot_general(
        newest, wdts[...], (((1,), (1,)), ((), ())), preferred_element_type=F32)[0:1])
    new_steps = softplus(new_raw + dtb_ref[...])
    head_s[...] = jnp.zeros_like(head_s)
    head_s[0:1, :] = new_steps
    head_s[1:2, :] = jnp.exp(-jnp.exp(alog_ref[...]) * new_steps)
    head_s[2:3, :] = dskip_ref[...]
    hrow = lax.broadcasted_iota(jnp.int32, (heads, hl * p_size), 0)
    hcol = lax.broadcasted_iota(jnp.int32, (heads, hl * p_size), 1)
    first = j * hl
    onehot = ((hcol >= (hrow - first) * p_size) & (hcol < (hrow - first + 1) * p_size)).astype(F32)
    spread_rows = jnp.dot(head_s[...], onehot, precision=lax.Precision.HIGHEST, preferred_element_type=F32)
    step_row, decay_row, skip_row = spread_rows[0:1], spread_rows[1:2], spread_rows[2:3]

    others(*pieces[len(order) - 2:])
    nears(*pieces[3:])

    def sent(s):
        for gp in range(PAIR):
            a_copy(s, gp).wait_send()
            pl.when(far)(b_copy(s, gp).wait_send)
            here, remote, _ = state_copy(s, gp)
            pl.when(jnp.logical_not(far) & jnp.logical_not(here))(remote.wait_send)

    pl.when(i != sp - 1)(halo.wait_send)

    @pl.when(i == sp - 1)
    def _():
        for r in range(spt):
            for q in range(tp):
                here, remote, _ = tail(r, q)
                pl.when(jnp.logical_not(here))(remote.wait_send)

    for k in range(sp):
        pl.when(i != k)(tot(k).wait_send)
    for s in range(steps):
        sent(s)
    for g in range(gl):
        for k in range(pairs + 1):
            pltpu.make_async_remote_copy(
                src_ref=st_out.at[0, 0], dst_ref=st_in.at[k, g], send_sem=st_send.at[0, 0],
                recv_sem=st_recv.at[k, g], device_id={"sp": after, "tp": j}, device_id_type=MESH).wait_recv()
        query = new_query[:, g * n_size:(g + 1) * n_size]
        key = new_keys[:, g * n_size:(g + 1) * n_size]
        query_rows = jnp.broadcast_to(query, (EDGE, n_size)).astype(BF16)
        held_row = sum(lax.dot_general(
            query_rows, st_in[k, g], (((1,), (1,)), ((), ())), preferred_element_type=F32)[0:1]
            for k in range(pairs + 1))
        for r in range(ratio):
            acc = sum(st_in[k, g, r * p_size:(r + 1) * p_size, :].astype(F32) for k in range(pairs + 1))
            state_ref[0, g * ratio + r] = acc.astype(BF16)
        span = slice(g * gcols, (g + 1) * gcols)
        inner_prod = jnp.sum(query * key, axis=1, keepdims=True)
        value_row = new_values[:, span]
        out = (decay_row[:, span] * held_row + (step_row[:, span] * inner_prod) * value_row
               + skip_row[:, span] * value_row)
        gated = out * silu(gate[:, span])
        ms = jnp.sum(gated * gated, axis=1, keepdims=True) / gcols
        normed = gated * lax.rsqrt(ms + EPS)
        for r in range(ratio):
            h = g * ratio + r
            read_s[h:h + 1, :] = normed[:, r * p_size:(r + 1) * p_size] * ng_ref[h:h + 1, :]
    read_ref[0] = read_s[...].astype(BF16)


def hand_over(state_in, read_in, state_out, read_out):
    state_out[...] = state_in[...]
    read_out[...] = read_in[...]


def per_device(
    dims, x_in, x_new, w_x, w_b, w_c, w_dt, w_z, conv_w, conv_b, dt_bias, a_log, d_skip, norm_g
):
    sp, tp, heads, groups, n_size, p_size, ratio, taps = dims
    spt, length, width = x_in.shape
    hl, gl = heads // tp, groups // tp
    assert x_new.shape[0] == 1 and sp == spt * tp and spt == 2 and sp % 4 == 0 and gl <= PAIR
    steps, gcols = groups // PAIR, ratio * p_size
    tiles = PAIR * (gcols + n_size) // LANES
    any_spec = pl.BlockSpec(memory_space=pl.ANY)
    vmem = pl.BlockSpec(memory_space=pltpu.VMEM)
    dma = pltpu.SemaphoreType.DMA
    results = pl.pallas_call(
        functools.partial(kernel, dims),
        out_shape=(
            pltpu.VMEM((1, hl, p_size, n_size), BF16),
            pltpu.VMEM((1, hl, p_size), BF16),
        ),
        in_specs=[any_spec, vmem] + [any_spec] * 7 + [vmem] * 4,
        out_specs=(vmem, vmem),
        scratch_shapes=[
            pltpu.VMEM((spt * length + EDGE, width), BF16),
            pltpu.VMEM((steps, width, PAIR * gcols), BF16),
            pltpu.VMEM((steps, width, PAIR * n_size), BF16),
            pltpu.VMEM((heads, width), BF16),
            pltpu.VMEM((width, gl * n_size), BF16),
            pltpu.VMEM((width, hl * p_size), BF16),
            pltpu.VMEM((2 * EDGE, width), BF16),
            pltpu.VMEM((tiles, SENT + length, LANES), F32),
            pltpu.VMEM((tiles, SENT + length, LANES), F32),
            pltpu.VMEM((tiles, SENT + length, LANES), F32),
            pltpu.VMEM((tiles, SENT + length, LANES), F32),
            pltpu.VMEM((tiles, SENT + length, LANES), F32),
            pltpu.VMEM((spt, length, LANES), F32),
            pltpu.VMEM((length, length), BF16),
            pltpu.VMEM((8, LANES), F32),
            pltpu.VMEM((spt, PAIR, length, n_size), BF16),
            pltpu.VMEM((spt, PAIR, gcols, length), BF16),
            pltpu.VMEM((spt, heads, length), F32),
            pltpu.VMEM((8, LANES), F32),
            pltpu.VMEM((sp, 8, LANES), F32),
            pltpu.VMEM((2, heads, LANES), F32),
            pltpu.VMEM((steps, PAIR, gcols, n_size), BF16),
            pltpu.VMEM((steps, PAIR, gcols, n_size), BF16),
            pltpu.VMEM((steps, PAIR, gcols, n_size), F32),
            pltpu.VMEM((steps, PAIR, gcols, n_size), BF16),
            pltpu.VMEM((steps, PAIR, gcols, n_size), BF16),
            pltpu.VMEM((sp // 4 + 1, gl, gcols, n_size), BF16),
            pltpu.VMEM((8, heads), F32),
            pltpu.VMEM((hl, p_size), F32),
            pltpu.VMEM(conv_w.shape, F32),
            pltpu.VMEM((1, conv_w.shape[1]), F32),
            pltpu.VMEM((SENT, width), BF16),
            dma((spt,)), dma, dma((steps, 2)), dma((2,)), dma((2,)), dma((1,)), dma((1,)),
            dma((spt, tp)), dma((1,)), dma((sp,)), dma((sp,)), dma((steps, PAIR)), dma((steps, PAIR)),
            dma((steps, PAIR)), dma((steps, PAIR)), dma((steps, PAIR)), dma((sp // 4 + 1, gl)),
        ],
        compiler_params=pltpu.CompilerParams(
            collective_id=0, has_side_effects=True, vmem_limit_bytes=60 * 1024 * 1024
        ),
    )(
        x_in, x_new, w_x, w_b, w_c, w_dt.T, w_z, conv_w, conv_b.reshape(1, -1),
        dt_bias.reshape(1, -1), a_log.reshape(1, -1), d_skip.reshape(1, -1), norm_g,
    )
    return pl.pallas_call(
        hand_over,
        out_shape=tuple(jax.ShapeDtypeStruct(r.shape, r.dtype) for r in results),
        in_specs=[vmem, vmem],
        out_specs=(vmem, vmem),
        compiler_params=pltpu.CompilerParams(vmem_limit_bytes=4 * 1024 * 1024),
    )(*results)


def solution(mesh):
    sp, tp = mesh.shape["sp"], mesh.shape["tp"]

    def step(x_in, x_new, w_x, w_b, w_c, w_dt, w_z, conv_w, conv_b, dt_bias, a_log, d_skip, norm_g):
        heads, p_size = w_dt.shape[1], norm_g.shape[1]
        keys_all = w_b.shape[1]
        n_size = LANES
        groups = keys_all // n_size
        dims = (sp, tp, heads, groups, n_size, p_size, heads // groups, conv_w.shape[0])
        return per_device(
            dims, x_in, x_new, w_x, w_b, w_c, w_dt, w_z, conv_w, conv_b, dt_bias, a_log, d_skip, norm_g)

    return jax.shard_map(
        step,
        mesh=mesh,
        in_specs=(
            P("tp", "sp", None), P("sp", None), P(), P(), P(), P(), P(None, "tp"),
            P(), P(), P(), P(), P(), P("tp", None),
        ),
        out_specs=(P("sp", "tp", None, None), P("sp", "tp", None)),
        check_vma=False,
    )
```

```python
import functools

import jax
import jax.numpy as jnp
from jax import lax
from jax.experimental import pallas as pl
from jax.experimental.pallas import tpu as pltpu
from jax.sharding import PartitionSpec as P

MESH = pl.DeviceIdType.MESH
F32 = jnp.float32
BF16 = jnp.bfloat16
EPS = 1e-05
EDGE = 16
SENT = 8
HALF = 4
PAIR = 2
LANES = 128


def silu(x):
    half = 0.5 * x
    return half + half * jnp.tanh(half)


def silu_twice(half):
    return half + half * jnp.tanh(half)


def softplus(x):
    return jnp.maximum(x, 0.0) + jnp.log1p(jnp.exp(-jnp.abs(x)))


def rounded(x):
    return x.astype(BF16).astype(F32)


def kernel(
    dims,
    x_ref, xn_ref, wx_ref, wb_ref, wc_ref, wdt_ref, wz_ref,
    cw_hbm, cb_hbm, dtb_ref, alog_ref, dskip_ref, ng_ref,
    state_ref, read_ref,
    xs, wxs, wbs, wdts, wcn, wzn, nt, pre_s0, pre_s1, pre_o0, pre_o1, pre_o2, padded, later, rows, keys, scaled,
    wt, tot_out, tot_in, fcol, a_out, a_in, mine, b_in, st_out, st_in, head_s, read_s, cw_ref, cb_ref, edges,
    x_sem, wdt_sem, w_sem, new_sem, conv_sem, halo_send, halo_recv, tail_send, tail_recv,
    tot_send, tot_recv, a_send, a_recv, b_send, b_recv, st_send, st_recv,
):
    sp, tp, heads, groups, n_size, p_size, ratio, taps = dims
    i, j = lax.axis_index("sp"), lax.axis_index("tp")
    spt, length, _ = x_ref.shape
    hl, gl = heads // tp, groups // tp
    inner, keys_all = heads * p_size, groups * n_size
    gcols = ratio * p_size
    steps = groups // PAIR
    home = i // spt
    pres = ((pre_s0, pre_s1), (pre_o0, pre_o1, pre_o2))
    member, m = lax.rem(i, 2), i // 2
    direct = m // 2 == j // 2
    near = jnp.logical_not(direct) & ((j > m) == (lax.rem(m, 2) == 1))
    far = jnp.logical_not(direct) & jnp.logical_not(near)
    partner, sibling = i + 1 - 2 * member, i + 2 - 4 * lax.rem(m, 2)
    pairs = sp // 4
    after = lax.rem(i + 1, sp)
    starts = (0, length + EDGE)
    seqs = (1 - member, member)
    width_v, width_k, width_h = PAIR * gcols, PAIR * n_size, PAIR * ratio
    vtiles, ktiles = width_v // LANES, width_k // LANES
    tiles_group = gcols // LANES
    heads_tile = LANES // p_size

    def place(s):
        return lax.rem(s + 1 + steps // 2 + (j * gl) // PAIR, steps)

    x_copies = [
        pltpu.make_async_copy(x_ref.at[seqs[r]], xs.at[pl.ds(starts[r], length)], x_sem.at[r])
        for r in range(spt)
    ]
    wdt_copy = pltpu.make_async_copy(wdt_ref, wdts, wdt_sem)

    def w_copies(s):
        at = place(s)
        return (
            pltpu.make_async_copy(
                wx_ref.at[:, pl.ds(pl.multiple_of(at * width_v, LANES), width_v)], wxs.at[s], w_sem.at[s, 0]),
            pltpu.make_async_copy(
                wb_ref.at[:, pl.ds(pl.multiple_of(at * width_k, LANES), width_k)], wbs.at[s], w_sem.at[s, 1]),
        )

    vcol = pl.multiple_of(j * (hl * p_size), LANES)
    gcol = pl.multiple_of(j * (gl * n_size), LANES)
    new_copies = [
        pltpu.make_async_copy(wc_ref.at[:, pl.ds(gcol, gl * n_size)], wcn, new_sem.at[0]),
        pltpu.make_async_copy(wz_ref, wzn, new_sem.at[1]),
    ]
    conv_copies = [
        pltpu.make_async_copy(cw_hbm, cw_ref, conv_sem.at[0]),
        pltpu.make_async_copy(cb_hbm, cb_ref, conv_sem.at[1]),
    ]
    x_copies[0].start()
    wdt_copy.start()
    x_copies[1].start()

    barrier = pltpu.get_barrier_semaphore()
    for k in range(sp):
        @pl.when(i != k)
        def _():
            pl.semaphore_signal(barrier, inc=1, device_id={"sp": k, "tp": j}, device_id_type=MESH)

        @pl.when(home != j)
        def _():
            pl.semaphore_signal(barrier, inc=1, device_id={"sp": k, "tp": home}, device_id_type=MESH)
    for c in w_copies(0):
        c.start(priority=1)
    for c in conv_copies:
        c.start()

    nt[0:EDGE - SENT, :] = jnp.zeros((EDGE - SENT, nt.shape[1]), BF16)
    padded[...] = jnp.zeros_like(padded)
    rows[...] = jnp.zeros_like(rows)
    for r in range(spt):
        rows[0:1, r * heads:(r + 1) * heads] = -jnp.exp(alog_ref[...])
        rows[1:2, r * heads:(r + 1) * heads] = dtb_ref[...]

    xs[length + SENT:length + EDGE, :] = jnp.zeros((EDGE - SENT, xs.shape[1]), BF16)

    @pl.when(i == 0)
    def _():
        xs[length:length + SENT, :] = jnp.zeros((SENT, xs.shape[1]), BF16)

    before = lax.broadcasted_iota(jnp.int32, (length, length), 0)
    column_at = lax.broadcasted_iota(jnp.int32, (length, length), 1)
    later[...] = (before > column_at).astype(F32).astype(BF16)

    def column(row):
        return jnp.broadcast_to(row, (LANES, LANES)).T

    def raw_steps(r):
        for lo in range(0, length, length // 2):
            raw = lax.dot_general(
                xs[starts[r] + lo:starts[r] + lo + length // 2, :], wdts[...], (((1,), (1,)), ((), ())),
                preferred_element_type=F32)
            padded[r, lo:lo + length // 2, 0:heads] = rounded(raw)

    x_copies[0].wait()
    wdt_copy.wait()
    raw_steps(0)
    x_copies[1].wait()
    lasts = [xs[starts[r] + length - EDGE:starts[r] + length, :].astype(F32) for r in range(spt)]
    edges[...] = jnp.concatenate([lasts[1][EDGE - HALF:], lasts[0][EDGE - HALF:]], axis=0).astype(BF16)
    pl.semaphore_wait(barrier, sp - 1 + spt * (tp - 1))

    halo = pltpu.make_async_remote_copy(
        src_ref=edges, dst_ref=xs.at[pl.ds(length, SENT)], send_sem=halo_send.at[0], recv_sem=halo_recv.at[0],
        device_id={"sp": after, "tp": j}, device_id_type=MESH)

    def tail(r, q):
        src = xs.at[pl.ds(starts[r] + length - SENT, SENT)]
        dst = nt.at[pl.ds(EDGE - SENT, SENT)]
        target = spt * j + seqs[r]
        return (target == i) & (q == j), pltpu.make_async_remote_copy(
            src_ref=src, dst_ref=dst, send_sem=tail_send.at[r, q], recv_sem=tail_recv.at[0],
            device_id={"sp": target, "tp": q}, device_id_type=MESH
        ), pltpu.make_async_copy(src, dst, tail_recv.at[0])

    pl.when(i != sp - 1)(halo.start)

    @pl.when(i == sp - 1)
    def _():
        for r in range(spt):
            for q in range(tp):
                here, remote, local = tail(r, q)
                pl.when(jnp.logical_not(here))(remote.start)
                pl.when(here)(local.start)

    raw_steps(1)

    def tot(k):
        return pltpu.make_async_remote_copy(
            src_ref=tot_out, dst_ref=tot_in.at[i], send_sem=tot_send.at[k], recv_sem=tot_recv.at[i],
            device_id={"sp": k, "tp": j}, device_id_type=MESH)

    def decays():
        turned = jnp.concatenate([padded[r].T[0:heads] for r in range(spt)], axis=0)
        rates = column(rows[0:1, :])[0:spt * heads, 0:1]
        biases = column(rows[1:2, :])[0:spt * heads, 0:1]
        sizes = softplus(turned + biases)
        parts, left = [], sizes
        for _ in range(3):
            parts.append(left.astype(BF16))
            left = left - parts[-1].astype(F32)
        sums = jnp.dot(jnp.concatenate(parts, axis=0), later[...], preferred_element_type=F32)
        rest = sum(sums[k * spt * heads:(k + 1) * spt * heads] for k in range(3))
        weights = jnp.exp(rates * rest) * sizes
        for r in range(spt):
            wt[r] = weights[r * heads:(r + 1) * heads]
        total = jnp.broadcast_to(rest[:, 0:1] + sizes[:, 0:1], (spt * heads, LANES))
        given, kept = total[0:heads], total[heads:2 * heads]
        tots = jnp.concatenate([
            jnp.where(member == 0, kept, given), jnp.where(member == 0, given, kept),
            jnp.zeros((LANES - spt * heads, LANES), F32)], axis=0)
        tot_out[...] = tots.T[0:8]

    def factors():
        for k in range(sp):
            @pl.when(i != k)
            def _():
                pltpu.make_async_remote_copy(
                    src_ref=tot_out, dst_ref=tot_in.at[k], send_sem=tot_send.at[k], recv_sem=tot_recv.at[k],
                    device_id={"sp": k, "tp": j}, device_id_type=MESH).wait_recv()
        for at, who in enumerate((i, partner)):
            beyond = jnp.zeros((1, LANES), F32)
            for k in range(sp):
                beyond = beyond + jnp.where(k > who, tot_in[k, 0:1, :], 0.0)
            both = column(jnp.exp(rows[0:1, :] * beyond))
            fcol[at] = jnp.where(member == 0, both[0:heads], both[heads:2 * heads])

    def a_copy(s, gp):
        return pltpu.make_async_remote_copy(
            src_ref=a_out.at[s, gp], dst_ref=a_in.at[s, gp], send_sem=a_send.at[s, gp], recv_sem=a_recv.at[s, gp],
            device_id={"sp": partner, "tp": j}, device_id_type=MESH)

    def b_copy(s, gp):
        return pltpu.make_async_remote_copy(
            src_ref=st_out.at[s, gp], dst_ref=b_in.at[s, gp], send_sem=b_send.at[s, gp], recv_sem=b_recv.at[s, gp],
            device_id={"sp": sibling, "tp": j}, device_id_type=MESH)

    slot = jnp.where(direct & (lax.rem(m, 2) == 1), pairs, m // 2)

    def state_copy(s, gp):
        g = place(s) * PAIR + gp
        q = g // gl
        src, dst = st_out.at[s, gp], st_in.at[slot, lax.rem(g, gl)]
        sem = st_recv.at[slot, lax.rem(g, gl)]
        return (m == j) & (q == j), pltpu.make_async_remote_copy(
            src_ref=src, dst_ref=dst, send_sem=st_send.at[s, gp], recv_sem=sem,
            device_id={"sp": spt * j + member, "tp": q}, device_id_type=MESH
        ), pltpu.make_async_copy(src, dst, sem)

    def pass_on(joined, s, gp):
        at = pl.multiple_of(place(s) * width_h, width_h)

        def add(gp, *more):
            scales = [fcol[k, pl.ds(at, width_h), :] for k in range(2)]
            for r in range(ratio):
                h, span = gp * ratio + r, slice(r * p_size, (r + 1) * p_size)
                total = scales[0][h:h + 1] * mine[s, gp, span, :]
                total += scales[1][h:h + 1] * a_in[s, gp, span, :].astype(F32)
                for ref in more:
                    total += ref[s, gp, span, :].astype(F32)
                st_out[s, gp, span, :] = total.astype(BF16)

        a_copy(s, gp).wait_recv()
        if joined:
            b_copy(s, gp).wait_recv()
            add(gp, b_in)
        else:
            add(gp)
            pl.when(far)(b_copy(s, gp).start)

        @pl.when(jnp.logical_not(far))
        def _():
            here, remote, local = state_copy(s, gp)
            pl.when(jnp.logical_not(here))(remote.start)
            pl.when(here)(local.start)

    def project(s, first, count, w, base, tiles, keep):
        cuts = [0, count] if tiles > 2 else [0, count // 2 // EDGE * EDGE, count]
        out = jnp.concatenate([
            jnp.dot(xs[first + lo:first + hi, :], w[s], preferred_element_type=F32)
            for lo, hi in zip(cuts, cuts[1:])], axis=0)
        for c in range(tiles):
            keep(base + c, out[:, c * LANES:(c + 1) * LANES])

    def given_alone(s):
        def keep(c, v):
            pres[0][s % 2][c, SENT:SENT + length, :] = v
        return s, 0, length, keep

    def given_with_edges(s):
        def keep(c, v):
            pres[0][s % 2][c, SENT:SENT + length, :] = v[0:length]
            pres[0][s % 2][c, HALF:SENT, :] = v[length:length + HALF]
            pres[1][s % 3][c, HALF:SENT, :] = v[length + HALF:length + SENT]
        return s, 0, length + EDGE, keep

    def kept_with_edges(s):
        def keep(c, v):
            pres[0][s % 2][c, HALF:SENT, :] = v[0:HALF]
            pres[1][s % 3][c, HALF:SENT, :] = v[HALF:SENT]
            pres[1][s % 3][c, SENT:SENT + length, :] = v[EDGE:EDGE + length]
        return s, length, length + EDGE, keep

    def kept_alone(s):
        def keep(c, v):
            pres[1][s % 3][c, SENT:SENT + length, :] = v
        return s, length + EDGE, length, keep

    def values_of(job):
        s, first, count, keep = job
        project(s, first, count, wxs, 0, vtiles, keep)

    def keys_of(job):
        s, first, count, keep = job
        project(s, first, count, wbs, vtiles, ktiles, keep)

    def contract(s, r, b):
        place_s = place(s)
        pre = pres[r][s % len(pres[r])]

        def conv(c):
            if c < vtiles:
                at = pl.multiple_of(place_s * width_v + c * LANES, LANES)
            else:
                at = pl.multiple_of(inner + place_s * width_k + (c - vtiles) * LANES, LANES)
            acc = cb_ref[:, pl.ds(at, LANES)]
            w = cw_ref[:, pl.ds(at, LANES)]
            for o in range(taps):
                acc = acc + w[o:o + 1] * pre[c, pl.ds(SENT - taps + 1 + o, length), :]
            return silu_twice(acc).astype(BF16)

        weights = wt[r, pl.ds(pl.multiple_of(place_s * width_h, width_h), width_h), :]
        for gp in range(PAIR):
            keys[b, gp] = conv(vtiles + gp)
            for c in range(gp * tiles_group, (gp + 1) * tiles_group):
                turned = conv(c).T
                for k in range(heads_tile):
                    h = c * heads_tile + k
                    part = turned[k * p_size:(k + 1) * p_size].astype(F32)
                    scaled[b, gp, (h - gp * ratio) * p_size:(h - gp * ratio + 1) * p_size] = (
                        weights[h:h + 1] * part).astype(BF16)

    def combine(s, r, b):
        outs = [jnp.dot(scaled[b, gp], keys[b, gp], preferred_element_type=F32) for gp in range(PAIR)]
        for gp in range(PAIR):
            if r == 0:
                a_out[s, gp] = outs[gp].astype(BF16)
            else:
                mine[s, gp] = outs[gp]
        if r == 0:
            for gp in range(PAIR):
                a_copy(s, gp).start()

    def w_wait(s):
        for c in w_copies(s):
            c.wait()

    w_wait(0)
    for c in w_copies(1):
        c.start()
    values_of(given_alone(0))
    decays()
    keys_of(given_alone(0))

    tot_in[i] = tot_out[...]
    for k in range(sp):
        pl.when(i != k)(tot(k).start)

    pl.when(i != 0)(halo.wait_recv)
    for s in range(2, steps):
        for c in w_copies(s):
            c.start()
    for c in new_copies:
        c.start()
    for c in conv_copies:
        c.wait()
    cw_ref[...] = 0.5 * cw_ref[...]
    cb_ref[...] = 0.5 * cb_ref[...]

    def block(job, turn):
        if turn is None:
            values_of(job)
            keys_of(job)
            return
        s, r, b = turn
        values_of(job)
        keys_of(job)
        contract(s, r, b)
        combine(s, r, b)

    def others(*pieces):
        for s, gp in pieces:
            pl.when(jnp.logical_not(near))(functools.partial(pass_on, False, s, gp))

    def nears(*pieces):
        for s, gp in pieces:
            pl.when(near)(functools.partial(pass_on, True, s, gp))

    order = [(0, 0), (0, 1)]
    for s in range(1, steps):
        order += [(s, 0), (s, 1)]
    pieces = [(s, gp) for s in range(steps) for gp in range(PAIR)]
    for k in range(1, len(order)):
        s, r = order[k]
        if r == 0:
            w_wait(s)
        job = kept_with_edges(0) if k == 1 else given_with_edges(s) if r == 0 else kept_alone(s)
        block(job, order[k - 1] + ((k - 1) % 2,))
        if k == 3:
            factors()
        if k >= 3:
            others(pieces[k - 3])
        if k == len(order) - 2:
            nears(*pieces[:2])
        if k == len(order) - 1:
            nears(pieces[2])
    others(pieces[len(order) - 3])

    newest = jnp.broadcast_to(xn_ref[...].astype(F32), (EDGE, xn_ref.shape[1])).astype(BF16)
    nt[EDGE:2 * EDGE, :] = newest
    tail(0, 0)[1].wait_recv()
    for c in new_copies:
        c.wait()

    s, r = order[-1]
    contract(s, r, (len(order) - 1) % 2)
    combine(s, r, (len(order) - 1) % 2)

    def new_conv(w, start, width):
        pre = rounded(jnp.dot(nt[...], w, preferred_element_type=F32))
        start = pl.multiple_of(start, LANES)
        acc = cb_ref[:, pl.ds(start, width)]
        w = cw_ref[:, pl.ds(start, width)]
        for o in range(taps):
            at = EDGE - taps + 1 + o
            acc = acc + w[o:o + 1] * pre[at:at + 1]
        return rounded(silu_twice(acc))

    skip = lax.rem(j * gl, PAIR)
    new_wx = wxs[steps // 2 - 1, :, pl.ds(pl.multiple_of(skip * gcols, LANES), hl * p_size)]
    new_wb = wbs[steps // 2 - 1, :, pl.ds(pl.multiple_of(skip * n_size, LANES), gl * n_size)]
    new_values = new_conv(new_wx, vcol, hl * p_size)
    new_keys = new_conv(new_wb, inner + gcol, gl * n_size)
    new_query = new_conv(wcn[...], inner + keys_all + gcol, gl * n_size)
    gate = rounded(jnp.dot(newest, wzn[...], preferred_element_type=F32)[0:1])
    new_raw = rounded(lax.dot_general(
        newest, wdts[...], (((1,), (1,)), ((), ())), preferred_element_type=F32)[0:1])
    new_steps = softplus(new_raw + dtb_ref[...])
    head_s[...] = jnp.zeros_like(head_s)
    head_s[0:1, :] = new_steps
    head_s[1:2, :] = jnp.exp(-jnp.exp(alog_ref[...]) * new_steps)
    head_s[2:3, :] = dskip_ref[...]
    hrow = lax.broadcasted_iota(jnp.int32, (heads, hl * p_size), 0)
    hcol = lax.broadcasted_iota(jnp.int32, (heads, hl * p_size), 1)
    first = j * hl
    onehot = ((hcol >= (hrow - first) * p_size) & (hcol < (hrow - first + 1) * p_size)).astype(F32)
    spread_rows = jnp.dot(head_s[...], onehot, precision=lax.Precision.HIGHEST, preferred_element_type=F32)
    step_row, decay_row, skip_row = spread_rows[0:1], spread_rows[1:2], spread_rows[2:3]

    others(*pieces[len(order) - 2:])
    nears(*pieces[3:])

    def sent(s):
        for gp in range(PAIR):
            a_copy(s, gp).wait_send()
            pl.when(far)(b_copy(s, gp).wait_send)
            here, remote, _ = state_copy(s, gp)
            pl.when(jnp.logical_not(far) & jnp.logical_not(here))(remote.wait_send)

    pl.when(i != sp - 1)(halo.wait_send)

    @pl.when(i == sp - 1)
    def _():
        for r in range(spt):
            for q in range(tp):
                here, remote, _ = tail(r, q)
                pl.when(jnp.logical_not(here))(remote.wait_send)

    for k in range(sp):
        pl.when(i != k)(tot(k).wait_send)
    for s in range(steps):
        sent(s)
    for g in range(gl):
        for k in range(pairs + 1):
            pltpu.make_async_remote_copy(
                src_ref=st_out.at[0, 0], dst_ref=st_in.at[k, g], send_sem=st_send.at[0, 0],
                recv_sem=st_recv.at[k, g], device_id={"sp": after, "tp": j}, device_id_type=MESH).wait_recv()
        query = new_query[:, g * n_size:(g + 1) * n_size]
        key = new_keys[:, g * n_size:(g + 1) * n_size]
        query_rows = jnp.broadcast_to(query, (EDGE, n_size)).astype(BF16)
        held_row = sum(lax.dot_general(
            query_rows, st_in[k, g], (((1,), (1,)), ((), ())), preferred_element_type=F32)[0:1]
            for k in range(pairs + 1))
        for r in range(ratio):
            acc = sum(st_in[k, g, r * p_size:(r + 1) * p_size, :].astype(F32) for k in range(pairs + 1))
            state_ref[0, g * ratio + r] = acc.astype(BF16)
        span = slice(g * gcols, (g + 1) * gcols)
        inner_prod = jnp.sum(query * key, axis=1, keepdims=True)
        value_row = new_values[:, span]
        out = (decay_row[:, span] * held_row + (step_row[:, span] * inner_prod) * value_row
               + skip_row[:, span] * value_row)
        gated = out * silu(gate[:, span])
        ms = jnp.sum(gated * gated, axis=1, keepdims=True) / gcols
        normed = gated * lax.rsqrt(ms + EPS)
        for r in range(ratio):
            h = g * ratio + r
            read_s[h:h + 1, :] = normed[:, r * p_size:(r + 1) * p_size] * ng_ref[h:h + 1, :]
    read_ref[0] = read_s[...].astype(BF16)


def hand_over(state_in, read_in, state_out, read_out):
    state_out[...] = state_in[...]
    read_out[...] = read_in[...]


def per_device(
    dims, x_in, x_new, w_x, w_b, w_c, w_dt, w_z, conv_w, conv_b, dt_bias, a_log, d_skip, norm_g
):
    sp, tp, heads, groups, n_size, p_size, ratio, taps = dims
    spt, length, width = x_in.shape
    hl, gl = heads // tp, groups // tp
    assert x_new.shape[0] == 1 and sp == spt * tp and spt == 2 and sp % 4 == 0 and gl <= PAIR
    steps, gcols = groups // PAIR, ratio * p_size
    tiles = PAIR * (gcols + n_size) // LANES
    any_spec = pl.BlockSpec(memory_space=pl.ANY)
    vmem = pl.BlockSpec(memory_space=pltpu.VMEM)
    dma = pltpu.SemaphoreType.DMA
    results = pl.pallas_call(
        functools.partial(kernel, dims),
        out_shape=(
            pltpu.VMEM((1, hl, p_size, n_size), BF16),
            pltpu.VMEM((1, hl, p_size), BF16),
        ),
        in_specs=[any_spec, vmem] + [any_spec] * 7 + [vmem] * 4,
        out_specs=(vmem, vmem),
        scratch_shapes=[
            pltpu.VMEM((spt * length + EDGE, width), BF16),
            pltpu.VMEM((steps, width, PAIR * gcols), BF16),
            pltpu.VMEM((steps, width, PAIR * n_size), BF16),
            pltpu.VMEM((heads, width), BF16),
            pltpu.VMEM((width, gl * n_size), BF16),
            pltpu.VMEM((width, hl * p_size), BF16),
            pltpu.VMEM((2 * EDGE, width), BF16),
            pltpu.VMEM((tiles, SENT + length, LANES), F32),
            pltpu.VMEM((tiles, SENT + length, LANES), F32),
            pltpu.VMEM((tiles, SENT + length, LANES), F32),
            pltpu.VMEM((tiles, SENT + length, LANES), F32),
            pltpu.VMEM((tiles, SENT + length, LANES), F32),
            pltpu.VMEM((spt, length, LANES), F32),
            pltpu.VMEM((length, length), BF16),
            pltpu.VMEM((8, LANES), F32),
            pltpu.VMEM((spt, PAIR, length, n_size), BF16),
            pltpu.VMEM((spt, PAIR, gcols, length), BF16),
            pltpu.VMEM((spt, heads, length), F32),
            pltpu.VMEM((8, LANES), F32),
            pltpu.VMEM((sp, 8, LANES), F32),
            pltpu.VMEM((2, heads, LANES), F32),
            pltpu.VMEM((steps, PAIR, gcols, n_size), BF16),
            pltpu.VMEM((steps, PAIR, gcols, n_size), BF16),
            pltpu.VMEM((steps, PAIR, gcols, n_size), F32),
            pltpu.VMEM((steps, PAIR, gcols, n_size), BF16),
            pltpu.VMEM((steps, PAIR, gcols, n_size), BF16),
            pltpu.VMEM((sp // 4 + 1, gl, gcols, n_size), BF16),
            pltpu.VMEM((8, heads), F32),
            pltpu.VMEM((hl, p_size), F32),
            pltpu.VMEM(conv_w.shape, F32),
            pltpu.VMEM((1, conv_w.shape[1]), F32),
            pltpu.VMEM((SENT, width), BF16),
            dma((spt,)), dma, dma((steps, 2)), dma((2,)), dma((2,)), dma((1,)), dma((1,)),
            dma((spt, tp)), dma((1,)), dma((sp,)), dma((sp,)), dma((steps, PAIR)), dma((steps, PAIR)),
            dma((steps, PAIR)), dma((steps, PAIR)), dma((steps, PAIR)), dma((sp // 4 + 1, gl)),
        ],
        compiler_params=pltpu.CompilerParams(
            collective_id=0, has_side_effects=True, vmem_limit_bytes=60 * 1024 * 1024
        ),
    )(
        x_in, x_new, w_x, w_b, w_c, w_dt.T, w_z, conv_w, conv_b.reshape(1, -1),
        dt_bias.reshape(1, -1), a_log.reshape(1, -1), d_skip.reshape(1, -1), norm_g,
    )
    return pl.pallas_call(
        hand_over,
        out_shape=tuple(jax.ShapeDtypeStruct(r.shape, r.dtype) for r in results),
        in_specs=[vmem, vmem],
        out_specs=(vmem, vmem),
        compiler_params=pltpu.CompilerParams(vmem_limit_bytes=4 * 1024 * 1024),
    )(*results)


def solution(mesh):
    sp, tp = mesh.shape["sp"], mesh.shape["tp"]

    def step(x_in, x_new, w_x, w_b, w_c, w_dt, w_z, conv_w, conv_b, dt_bias, a_log, d_skip, norm_g):
        heads, p_size = w_dt.shape[1], norm_g.shape[1]
        keys_all = w_b.shape[1]
        n_size = LANES
        groups = keys_all // n_size
        dims = (sp, tp, heads, groups, n_size, p_size, heads // groups, conv_w.shape[0])
        return per_device(
            dims, x_in, x_new, w_x, w_b, w_c, w_dt, w_z, conv_w, conv_b, dt_bias, a_log, d_skip, norm_g)

    return jax.shard_map(
        step,
        mesh=mesh,
        in_specs=(
            P("tp", "sp", None), P("sp", None), P(), P(), P(), P(), P(None, "tp"),
            P(), P(), P(), P(), P(), P("tp", None),
        ),
        out_specs=(P("sp", "tp", None, None), P("sp", "tp", None)),
        check_vma=False,
    )
```
